32 devices in a mesh: sp: 16 (over z, y, x), tp: 2 (over core).
Axes of the slice: x: 2, y: 2, z: 4, core: 2. Of those that a mesh axis runs over, the one named last changes fastest.
Arguments:
- resid: bfloat16 [3072, 2048], P('sp'), may hold values from -6 to 6
- queries: bfloat16 [3072, 1024], P('sp', 'tp'), may hold values from -6.5 to 6.5
- keys: bfloat16 [3072, 1024], P('sp', 'tp'), may hold values from -6.5 to 6.5
- values: bfloat16 [3072, 1024], P('sp', 'tp'), may hold values from -6 to 6
- lambdas: float32 [8], P('tp'), may hold values from 0.3 to 0.8
- head_gain: float32 [128], replicated, may hold values from 0.1 to 1.9
- out_weight: bfloat16 [1024, 2048], P('tp'), may hold values from -0.1875 to 0.1875
- norm_gain: float32 [2048], replicated, may hold values from 0.1 to 1.9
- gate_weight: bfloat16 [2048, 5632], P('sp', 'tp'), may hold values from -0.125 to 0.125
- up_weight: bfloat16 [2048, 5632], P('sp', 'tp'), may hold values from -0.125 to 0.125
- down_weight: bfloat16 [5632, 2048], P('tp', 'sp'), may hold values from -0.078125 to 0.078125
Outputs:
- result: bfloat16 [3072, 2048], P('sp')
The draws below stay inside these ranges and needn't reach their ends.
All inputs are finite; a program needn't handle non-finite values.
Results may differ from the reference program's by a relative error of at most 0.014.
Values may be sent and summed in bfloat16 or wider, within the bound.
A program may use at most 128 MiB of HBM per device.

```python
import jax
import jax.numpy as jnp
from jax import lax

D = 2048
HEADS = 8
QK = 64
VD = 128
FF = 5632
TOK_DEV = 192
TOKENS = 3072
N_TP = 2


def shared_field(key, salt, planted_row, period):
    width = HEADS * 2 * QK
    field = jnp.clip(jax.random.normal(jax.random.fold_in(key, salt), (TOKENS, width), jnp.float32) * 1.3, -6.5, 6.5)
    return field


def draw_queries(key, part):
    return shared_field(key, 11, 5, 97).astype(jnp.bfloat16)


def draw_keys(key, part):
    return shared_field(key, 23, 3, 89).astype(jnp.bfloat16)


def level_of(own_key, shape, cuts, low, high):
    factor_of, own = 1.0, jax.random.fold_in(own_key, 6)
    for position, blocks in cuts:
        steps = jnp.exp(jax.random.uniform(jax.random.fold_in(own, position), (blocks,), jnp.float32, low / len(cuts), high / len(cuts)))
        factor_of = factor_of * jnp.repeat(steps, shape[position] // blocks).reshape([-1 if axis == position else 1 for axis in range(len(shape))])
    return factor_of


def normal_values(stream_key, extent, scale, bound, cuts=(), kind=jnp.bfloat16):
    gain = level_of(stream_key, extent, cuts, -0.22, 0.18) if cuts else 1.0
    array = jax.random.normal(stream_key, extent, jnp.float32) * scale * gain
    return jnp.minimum(jnp.maximum(array, -bound), bound).astype(kind)


def setup_inputs(seed: int = 0) -> dict:
    splits = jax.random.split(jax.random.key(seed), 12)
    resid = normal_values(splits[0], (TOKENS, D), 1.0, 6.0, ((0, 16),))
    queries = draw_queries(jax.random.fold_in(splits[11], 71), 0)
    keys = draw_keys(jax.random.fold_in(splits[11], 71), 0)
    values = normal_values(splits[3], (TOKENS, HEADS * VD), 1.0, 6.0, ((0, 16), (1, 2)))
    lambdas = jnp.clip(0.3 + 0.5 * jax.random.uniform(splits[4], (HEADS,), jnp.float32) ** level_of(splits[4], (HEADS,), ((0, 2),), -0.2, 0.2), 0.3, 0.8)
    head_gain = jnp.clip(1.0 + 0.18 * jax.random.normal(splits[5], (VD,), jnp.float32), 0.1, 1.9)
    out_weight = normal_values(splits[6], (HEADS * VD, D), (HEADS * VD) ** -0.5, 0.1875, ((0, 2),))
    norm_gain = jnp.clip(1.0 + 0.18 * jax.random.normal(splits[7], (D,), jnp.float32), 0.1, 1.9)
    gate_weight = normal_values(splits[8], (D, FF), D ** -0.5, 0.125, ((0, 16), (1, 2)))
    up_weight = normal_values(splits[9], (D, FF), D ** -0.5, 0.125, ((0, 16), (1, 2)))
    down_weight = normal_values(splits[10], (FF, D), FF ** -0.5, 0.078125, ((0, 2), (1, 16)))
    return dict(resid=resid, queries=queries, keys=keys, values=values, lambdas=lambdas, head_gain=head_gain, out_weight=out_weight, norm_gain=norm_gain, gate_weight=gate_weight, up_weight=up_weight, down_weight=down_weight)


def reference(resid, queries, keys, values, lambdas, head_gain, out_weight, norm_gain, gate_weight, up_weight, down_weight):
    tok_total = resid.shape[0]
    head_count = lambdas.shape[0]
    query_all = queries.reshape(tok_total, head_count, 2, QK).astype(jnp.float32)
    key_all = keys.reshape(tok_total, head_count, 2, QK).astype(jnp.float32)
    value_all = values.reshape(tok_total, head_count, VD).astype(jnp.float32)
    score_scale = QK ** (-0.5)
    key_pos = jnp.arange(tok_total, dtype=jnp.int32)

    def one_block(block_index):
        block_start = (block_index * TOK_DEV).astype(jnp.int32)
        query_block = lax.dynamic_slice_in_dim(query_all, block_start, TOK_DEV, 0)
        scores = jnp.einsum('qhcd,khcd->chqk', query_block, key_all) * score_scale
        query_pos = block_start + jnp.arange(TOK_DEV, dtype=jnp.int32)
        causal_mask = key_pos[None, :] <= query_pos[:, None]
        scores = jnp.where(causal_mask, scores, -1e+30)
        row_max = lax.optimization_barrier(jnp.max(scores, axis=-1, keepdims=True))
        expo = jnp.where(causal_mask, jnp.exp(scores - row_max), 0.0)
        row_sum = lax.optimization_barrier(jnp.sum(expo, axis=-1))
        rounded = lax.optimization_barrier(expo.astype(jnp.bfloat16)).astype(jnp.float32)
        numer = jnp.einsum('chqk,khd->chqd', rounded, value_all)
        ratio = numer / row_sum[..., None]
        mixed_heads = ratio[0] - lambdas[:, None, None] * ratio[1]
        normed_heads = mixed_heads * lax.rsqrt(lax.optimization_barrier(jnp.mean(mixed_heads * mixed_heads, axis=-1, keepdims=True)) + 1e-05) * head_gain
        return jnp.transpose(normed_heads.astype(jnp.bfloat16), (1, 0, 2))
    head_out = lax.map(one_block, jnp.arange(tok_total // TOK_DEV, dtype=jnp.int32)).reshape(tok_total, head_count * VD)
    group_cols = head_count // N_TP * VD
    branch = jnp.zeros((tok_total, resid.shape[1]), jnp.float32)
    for group in range(N_TP):
        partial_sum = jnp.dot(head_out[:, group * group_cols:(group + 1) * group_cols], out_weight[group * group_cols:(group + 1) * group_cols], preferred_element_type=jnp.float32)
        branch = branch + partial_sum.astype(jnp.bfloat16).astype(jnp.float32)
    first = resid.astype(jnp.float32) + branch
    normed = (first * lax.rsqrt(lax.optimization_barrier(jnp.mean(first * first, axis=-1, keepdims=True)) + 1e-06) * norm_gain).astype(jnp.bfloat16)
    hidden_group = FF // N_TP
    mixer = jnp.zeros_like(first)
    for group in range(N_TP):
        cols = slice(group * hidden_group, (group + 1) * hidden_group)
        gate_act = jnp.dot(normed, gate_weight[:, cols], preferred_element_type=jnp.float32)
        up_act = jnp.dot(normed, up_weight[:, cols], preferred_element_type=jnp.float32)
        hidden = (jax.nn.silu(gate_act) * up_act).astype(jnp.bfloat16)
        partial_sum = jnp.dot(hidden, down_weight[cols, :], preferred_element_type=jnp.float32)
        mixer = mixer + partial_sum.astype(jnp.bfloat16).astype(jnp.float32)
    return (first + 0.5 * mixer).astype(jnp.bfloat16)
```

```python
import functools

import jax
import jax.numpy as jnp
from jax import lax
from jax.experimental import pallas as pl
from jax.experimental.pallas import tpu as pltpu
from jax.sharding import PartitionSpec as P

QK = 64
VD = 128
LANE = 128
VMEM_LIMIT = 60 * 1024 * 1024


def rms_rows(first, norm_gain):
    return (
        first * lax.rsqrt(jnp.mean(first * first, axis=-1, keepdims=True) + 1e-06) * norm_gain
    ).astype(jnp.bfloat16)


def generic(
    resid,
    queries,
    keys,
    values,
    lambdas,
    head_gain,
    out_weight,
    norm_gain,
    gate_weight,
    up_weight,
    down_weight,
):
    tok_rows = queries.shape[0]
    local_heads = lambdas.shape[0]
    model_width = resid.shape[1]
    offset = lax.axis_index("sp") * tok_rows
    query_four = queries.reshape(tok_rows, local_heads, 2, QK)
    score_scale = QK ** (-0.5)
    query_pos = offset + lax.iota(jnp.int32, tok_rows)

    def update(fold_state, key_part, value_part, key_pos):
        run_max, run_sum, run_acc = fold_state
        scores = (
            jnp.einsum("qhcd,khcd->chqk", query_four, key_part, preferred_element_type=jnp.float32)
            * score_scale
        )
        causal_mask = key_pos[None, :] <= query_pos[:, None]
        scores = jnp.where(causal_mask, scores, -1e30)
        new_max = jnp.maximum(run_max, jnp.max(scores, axis=-1))
        expo = jnp.where(causal_mask, jnp.exp(scores - new_max[..., None]), 0.0)
        factor = jnp.exp(run_max - new_max)
        new_sum = run_sum * factor + jnp.sum(expo, axis=-1)
        new_acc = run_acc * factor[..., None] + jnp.einsum(
            "chqk,khd->chqd",
            expo.astype(jnp.bfloat16),
            value_part,
            preferred_element_type=jnp.float32,
        )
        return (new_max, new_sum, new_acc)

    initial = (
        jnp.full((2, local_heads, tok_rows), -1e30, jnp.float32),
        jnp.zeros((2, local_heads, tok_rows), jnp.float32),
        jnp.zeros((2, local_heads, tok_rows, VD), jnp.float32),
    )
    key_rows = lax.all_gather(keys, "sp", axis=0, tiled=True)
    value_rows = lax.all_gather(values, "sp", axis=0, tiled=True)
    key_count = key_rows.shape[0]
    key_span = key_count
    while key_span > 1024 and key_span % 2 == 0:
        key_span = key_span // 2

    def one_span(span_index, inner_state):
        span_start = span_index * key_span
        key_part = lax.dynamic_slice_in_dim(key_rows, span_start, key_span, 0).reshape(
            key_span, local_heads, 2, QK
        )
        value_part = lax.dynamic_slice_in_dim(value_rows, span_start, key_span, 0).reshape(
            key_span, local_heads, VD
        )
        key_pos = span_start + lax.iota(jnp.int32, key_span)
        return update(inner_state, key_part, value_part, key_pos)

    final_max, final_sum, final_acc = lax.fori_loop(0, key_count // key_span, one_span, initial)
    ratio = final_acc / final_sum[..., None]
    mixed_heads = ratio[0] - lambdas[:, None, None] * ratio[1]
    head_out = (
        mixed_heads
        * lax.rsqrt(jnp.mean(mixed_heads * mixed_heads, axis=-1, keepdims=True) + 1e-05)
        * head_gain
    ).astype(jnp.bfloat16)
    out_three = out_weight.reshape(local_heads, VD, model_width)
    own_count = tok_rows // lax.axis_size("tp")
    branch = lax.psum_scatter(
        jnp.einsum("hqd,hde->qe", head_out, out_three, preferred_element_type=jnp.float32).astype(
            jnp.bfloat16
        ),
        "tp",
        scatter_dimension=0,
        tiled=True,
    ).astype(jnp.float32)
    resid_own = lax.dynamic_slice_in_dim(resid, lax.axis_index("tp") * own_count, own_count, 0)
    first = resid_own.astype(jnp.float32) + branch
    normed_all = lax.all_gather(rms_rows(first, norm_gain), "tp", axis=0, tiled=True)
    gate_act = jnp.dot(
        normed_all,
        lax.all_gather(gate_weight, "sp", axis=0, tiled=True),
        preferred_element_type=jnp.float32,
    )
    up_act = jnp.dot(
        normed_all,
        lax.all_gather(up_weight, "sp", axis=0, tiled=True),
        preferred_element_type=jnp.float32,
    )
    hidden = (jax.nn.silu(gate_act) * up_act).astype(jnp.bfloat16)
    terms = jnp.dot(
        hidden,
        lax.all_gather(down_weight, "sp", axis=1, tiled=True),
        preferred_element_type=jnp.float32,
    )
    mixer = lax.psum_scatter(
        terms.astype(jnp.bfloat16), "tp", scatter_dimension=0, tiled=True
    ).astype(jnp.float32)
    finished = (first + 0.5 * mixer).astype(jnp.bfloat16)
    return lax.all_gather(finished, "tp", axis=0, tiled=True)


def where_am_i(R):
    s = lax.axis_index("sp")
    return s // R, lax.rem(s, R), lax.axis_index("tp")


def remote(src, dst, send, recv, sp, tp):
    return pltpu.make_async_remote_copy(
        src_ref=src,
        dst_ref=dst,
        send_sem=send,
        recv_sem=recv,
        device_id={"sp": sp, "tp": tp},
        device_id_type=pl.DeviceIdType.MESH,
    )


def greet(peers):
    barrier = pltpu.get_barrier_semaphore()
    for sp, tp in peers:
        pl.semaphore_signal(
            barrier,
            inc=1,
            device_id={"sp": sp, "tp": tp},
            device_id_type=pl.DeviceIdType.MESH,
        )
    pl.semaphore_wait(barrier, len(peers))


def first_block(zz, share):
    return (zz * share) // LANE


def mirror_x(r):
    return r + 1 - 2 * lax.rem(r, 2)


def mirror_y(r):
    return r + 2 - 4 * (lax.rem(r, 4) // 2)


def gather_kernel(Z, R, share, width, ins, outs, sems):
    q_in, k_in, v_in, g_in, u_in, d_in = ins
    q_out, k_out, v_out, g_out, u_out, d_out = outs
    send1, recv1, send2, recv2, local_sem = sems
    z, r, t = where_am_i(R)
    rx, ry = mirror_x(r), mirror_y(r)
    rd = mirror_x(ry)
    T = k_in.shape[0]
    W = g_in.shape[0]

    def dev(zz, rr):
        return zz * R + rr

    greet([(dev(lax.rem(z + j, Z), r), t) for j in range(1, Z)] + [(dev(z, rx), t), (dev(z, ry), t)])

    def cols(zz):
        return pl.ds(pl.multiple_of(zz * VD, LANE), VD)

    def wide(zz):
        return pl.ds(pl.multiple_of(first_block(zz, share) * LANE, LANE), width)

    def source(a, zz, h=None):
        ref = (q_in, k_in, v_in, g_in, u_in, d_in)[a]
        if a == 5:
            start = pl.multiple_of(first_block(zz, share) * LANE, LANE)
            if h is None:
                return ref.at[pl.ds(start, width), :]
            n = width // 2
            return ref.at[pl.ds(pl.multiple_of(start + h * n, 64), n), :]
        rows = T if a < 3 else W
        sl = cols(zz) if a < 3 else wide(zz)
        if h is None:
            return ref.at[:, sl]
        n = rows // 2
        return ref.at[pl.ds(h * n, n), sl]

    def place(a, zz, rr, h=None):
        ref = (q_out, k_out, v_out, g_out, u_out, d_out)[a]
        if a == 0:
            return ref.at[zz]
        slot = dev(zz, rr)
        if h is None:
            return ref.at[slot]
        n = ref.shape[1] // 2
        return ref.at[slot, pl.ds(h * n, n), :]

    def first_hop(a, j):
        zz = lax.rem(z + j, Z)
        return remote(source(a, zz), place(a, z, r), send1.at[a, j], recv1.at[a, j], dev(zz, r), t)

    def arrived(a, j):
        zz = lax.rem(z + Z - j, Z)
        remote(source(a, z), place(a, zz, r), send1.at[a, j], recv1.at[a, j], dev(zz, r), t).wait_recv()

    started = []
    locals_ = []
    for group in ((1, 2, 0), (3, 4, 5)):
        for j in range(1, Z):
            for a in group:
                c = first_hop(a, j)
                c.start()
                started.append(c)
        for a in group:
            c = pltpu.make_async_copy(source(a, z), place(a, z, r), local_sem.at[a])
            c.start()
            locals_.append(c)

    def hop2(a, j, kind, owner, h, target, from_input):
        zz = lax.rem(z + Z - j, Z)
        src = source(a, z, h) if from_input else place(a, zz, owner, h)
        return remote(
            src,
            place(a, zz, owner, h),
            send2.at[a - 1, j, kind],
            recv2.at[a - 1, j, kind],
            dev(z, target),
            t,
        )

    def wait2(a, j, kind):
        owner = (rx, rx, ry, ry, rd, rd)[kind]
        h = (0, 1, 0, 1, 0, 1)[kind]
        target = (rx, rx, ry, ry, ry, rx)[kind]
        hop2(a, j, kind, owner, h, target, False).wait_recv()

    pieces = [(a, j) for j in range(Z) for a in (1, 2)] + [
        (a, j) for j in range(Z) for a in (3, 4, 5)
    ]
    lag = 2
    for i in range(len(pieces) + lag):
        if i < len(pieces):
            a, j = pieces[i]
            if j:
                arrived(a, j)
            for kind, h, target in ((0, 0, rx), (3, 1, ry), (1, 1, rx), (2, 0, ry)):
                c = hop2(a, j, kind, r, h, target, j == 0)
                c.start()
                started.append(c)
        if i >= lag:
            a, j = pieces[i - lag]
            wait2(a, j, 0)
            c = hop2(a, j, 4, rx, 0, ry, False)
            c.start()
            started.append(c)
            wait2(a, j, 3)
            c = hop2(a, j, 5, ry, 1, rx, False)
            c.start()
            started.append(c)
    for a, j in pieces:
        for kind in (1, 2, 4, 5):
            wait2(a, j, kind)
    for j in range(1, Z):
        arrived(0, j)
    for c in locals_:
        c.wait()
    for c in started:
        c.wait_send()


def gather_all(Z, R, q, k, v, g, u, d):
    T, W = k.shape[0], g.shape[0]
    share = g.shape[1] // Z
    width = max(
        -(-((zz + 1) * share) // LANE) - (zz * share) // LANE for zz in range(Z)
    ) * LANE
    S = Z * R

    def kernel(*refs):
        gather_kernel(Z, R, share, width, refs[:6], refs[6:12], refs[12:])

    bf = jnp.bfloat16
    return pl.pallas_call(
        kernel,
        out_shape=[
            jax.ShapeDtypeStruct((Z, T, VD), bf),
            jax.ShapeDtypeStruct((S, T, VD), bf),
            jax.ShapeDtypeStruct((S, T, VD), bf),
            jax.ShapeDtypeStruct((S, W, width), bf),
            jax.ShapeDtypeStruct((S, W, width), bf),
            jax.ShapeDtypeStruct((S, width, d.shape[1]), bf),
        ],
        in_specs=[pl.BlockSpec(memory_space=pltpu.VMEM)] * 6,
        out_specs=[pl.BlockSpec(memory_space=pl.ANY)] * 6,
        scratch_shapes=[
            pltpu.SemaphoreType.DMA((6, Z)),
            pltpu.SemaphoreType.DMA((6, Z)),
            pltpu.SemaphoreType.DMA((5, Z, 6)),
            pltpu.SemaphoreType.DMA((5, Z, 6)),
            pltpu.SemaphoreType.DMA((6,)),
        ],
        compiler_params=pltpu.CompilerParams(
            collective_id=0, has_side_effects=True, vmem_limit_bytes=VMEM_LIMIT
        ),
    )(q, k, v, g, u, d)


def attention_block(R, T, i, r, q_at, k_at, v_at, lam, gain):
    span = R * T
    query = q_at(i) * jnp.bfloat16(QK**-0.5)
    ratios = []
    for c in range(2):
        part = query[:, c * QK : (c + 1) * QK]

        def fold(n, state, masked):
            run_max, run_sum, run_acc = state
            key = k_at(n)[:, c * QK : (c + 1) * QK]
            scores = lax.dot_general(
                part, key, (((1,), (1,)), ((), ())), preferred_element_type=jnp.float32
            )
            if masked:
                qpos = r * T + lax.broadcasted_iota(jnp.int32, scores.shape, 0)
                kpos = lax.broadcasted_iota(jnp.int32, scores.shape, 1)
                scores = jnp.where(kpos <= qpos, scores, -1e30)
            new_max = jnp.maximum(run_max, jnp.max(scores, axis=-1, keepdims=True))
            expo = jnp.exp(scores - new_max)
            factor = jnp.exp(run_max - new_max)
            new_sum = run_sum * factor + jnp.sum(expo, axis=-1, keepdims=True)
            new_acc = run_acc * factor + jnp.dot(
                expo.astype(jnp.bfloat16), v_at(n), preferred_element_type=jnp.float32
            )
            return new_max, new_sum, new_acc

        state = (
            jnp.full((T, 1), -1e30, jnp.float32),
            jnp.zeros((T, 1), jnp.float32),
            jnp.zeros((T, VD), jnp.float32),
        )
        state = fold(i, state, True)
        state = lax.fori_loop(0, i, lambda n, st: fold(n, st, False), state)
        ratios.append(state[2] / state[1])
    mixed = ratios[0] - lam * ratios[1]
    return (
        mixed * lax.rsqrt(jnp.mean(mixed * mixed, axis=-1, keepdims=True) + 1e-05) * gain
    ).astype(jnp.bfloat16)


def attention_kernel(Z, R, q_ref, k_ref, v_ref, lam_ref, gain_ref, out_ref):
    z, r, _ = where_am_i(R)
    T = q_ref.shape[1]
    span = R * T
    lam = lam_ref[z]

    def at(ref, n):
        return ref[pl.ds(pl.multiple_of(n * span, span), span), :]

    @pl.loop(0, Z)
    def _(i):
        out_ref[i] = attention_block(
            R,
            T,
            i,
            r,
            lambda b: q_ref[b],
            lambda n: at(k_ref, n),
            lambda n: at(v_ref, n),
            lam,
            gain_ref[...],
        )


def attention(Z, R, q, k, v, lambdas, head_gain):
    vm = pl.BlockSpec(memory_space=pltpu.VMEM)
    return pl.pallas_call(
        functools.partial(attention_kernel, Z, R),
        out_shape=jax.ShapeDtypeStruct(q.shape, jnp.bfloat16),
        in_specs=[vm, vm, vm, pl.BlockSpec(memory_space=pltpu.SMEM), vm],
        out_specs=vm,
        compiler_params=pltpu.CompilerParams(vmem_limit_bytes=VMEM_LIMIT),
    )(q, k, v, lambdas, head_gain.reshape(1, -1))


def branch_kernel(
    Z, R, ho, resid, w, gain, first_ref, all_ref, heads, part, got, norm_sc, sem_a, sem_b, sem_c, sem_d, loc
):
    z, r, t = where_am_i(R)
    me = z * R + r
    T = resid.shape[0]
    H = T // 2
    greet([(lax.rem(z + j, Z) * R + r, t) for j in range(1, Z)] + [(me, 1 - t)])
    copies = []
    for j in range(1, Z):
        zz = lax.rem(z + j, Z)
        c = remote(ho.at[zz], heads.at[z], sem_a.at[0, j], sem_a.at[1, j], zz * R + r, t)
        c.start()
        copies.append(c)
    own = pltpu.make_async_copy(ho.at[z], heads.at[z], loc.at[0])
    own.start()
    own.wait()
    for c in copies:
        c.wait()
    D = w.shape[1]
    NT = 512 if D % 512 == 0 else D
    for h in range(2):
        hh = (1 - t) if h == 0 else t
        rows = pl.ds(pl.multiple_of(hh * H, 16), H)
        left = jnp.concatenate([heads[n, rows, :] for n in range(Z)], axis=1)
        for n in range(0, D, NT):
            part[h, :, n : n + NT] = jnp.dot(
                left, w[:, n : n + NT], preferred_element_type=jnp.float32
            ).astype(jnp.bfloat16)
        if h == 0:
            swap = remote(part.at[0], got, sem_b.at[0], sem_b.at[1], me, 1 - t)
            swap.start()
    swap.wait()
    own_rows = pl.ds(pl.multiple_of(t * H, 16), H)
    first = resid[own_rows, :].astype(jnp.float32) + (
        part[1].astype(jnp.float32) + got[...].astype(jnp.float32)
    )
    first_ref[...] = first
    norm_sc[...] = rms_rows(first, gain[...])

    def rows_of(zz, tt):
        return all_ref.at[pl.ds(pl.multiple_of(zz * T + tt * H, 16), H), :]

    copies = []
    for j in range(1, Z):
        zz = lax.rem(z + j, Z)
        c = remote(norm_sc, rows_of(z, t), sem_c.at[0, j], sem_c.at[1, j], zz * R + r, t)
        c.start()
        copies.append(c)
    across = [remote(norm_sc, rows_of(z, t), sem_d.at[0, 0], sem_d.at[1, 0], me, 1 - t)]
    across[0].start()
    own = pltpu.make_async_copy(norm_sc, rows_of(z, t), loc.at[1])
    own.start()
    for j in range(1, Z):
        zz = lax.rem(z + Z - j, Z)
        remote(norm_sc, rows_of(zz, t), sem_c.at[0, j], sem_c.at[1, j], zz * R + r, t).wait_recv()
        c = remote(rows_of(zz, t), rows_of(zz, t), sem_d.at[0, j], sem_d.at[1, j], me, 1 - t)
        c.start()
        across.append(c)
    own.wait()
    for c in copies:
        c.wait_send()
    for j in range(Z):
        zz = lax.rem(z + Z - j, Z)
        remote(
            rows_of(zz, t), rows_of(zz, 1 - t), sem_d.at[0, j], sem_d.at[1, j], me, 1 - t
        ).wait_recv()
    for c in across:
        c.wait_send()


def branch(Z, R, ho, resid, w, norm_gain):
    vm = pl.BlockSpec(memory_space=pltpu.VMEM)
    T, D = resid.shape
    H = T // 2
    return pl.pallas_call(
        functools.partial(branch_kernel, Z, R),
        out_shape=[
            jax.ShapeDtypeStruct((H, D), jnp.float32),
            jax.ShapeDtypeStruct((Z * T, D), jnp.bfloat16),
        ],
        in_specs=[vm] * 4,
        out_specs=[vm, vm],
        scratch_shapes=[
            pltpu.VMEM(ho.shape, jnp.bfloat16),
            pltpu.VMEM((2, H, D), jnp.bfloat16),
            pltpu.VMEM((H, D), jnp.bfloat16),
            pltpu.VMEM((H, D), jnp.bfloat16),
            pltpu.SemaphoreType.DMA((2, Z)),
            pltpu.SemaphoreType.DMA((2,)),
            pltpu.SemaphoreType.DMA((2, Z)),
            pltpu.SemaphoreType.DMA((2, Z)),
            pltpu.SemaphoreType.DMA((2,)),
        ],
        compiler_params=pltpu.CompilerParams(
            collective_id=1, has_side_effects=True, vmem_limit_bytes=VMEM_LIMIT
        ),
    )(ho, resid, w, norm_gain.reshape(1, -1))


def finish_kernel(Z, R, terms, first, out, cross, sums, landed, mine, sem_a, sem_b, sem_c, loc):
    z, r, t = where_am_i(R)
    me = z * R + r
    H = first.shape[0]
    greet([(lax.rem(z + j, Z) * R + r, t) for j in range(1, Z)] + [(me, 1 - t)])
    copies = []
    order = [j % Z for j in range(1, Z + 1)]
    for j in order:
        zz = lax.rem(z + j, Z)
        c = remote(
            terms.at[zz, 1 - t], cross.at[zz], sem_a.at[0, j], sem_a.at[1, j], me, 1 - t
        )
        c.start()
        copies.append(c)
    sent = []
    total = None
    for n, j in enumerate(order):
        zz = lax.rem(z + j, Z)
        copies[n].wait()
        total = terms[zz, t].astype(jnp.float32) + cross[zz].astype(jnp.float32)
        if j:
            sums[j] = total.astype(jnp.bfloat16)
            c = remote(sums.at[j], landed.at[j], sem_b.at[0, j], sem_b.at[1, j], zz * R + r, t)
            c.start()
            sent.append(c)
        else:
            mine[...] = total
    for c in sent:
        c.wait()
    total = mine[...]
    for j in range(1, Z):
        total = total + landed[j].astype(jnp.float32)
    rows = pl.ds(pl.multiple_of(t * H, 16), H)
    sums[0] = (first[...] + 0.5 * total).astype(jnp.bfloat16)
    c = remote(sums.at[0], out.at[rows, :], sem_c.at[0], sem_c.at[1], me, 1 - t)
    c.start()
    own = pltpu.make_async_copy(sums.at[0], out.at[rows, :], loc)
    own.start()
    own.wait()
    c.wait()


def finish(Z, R, terms, first):
    vm = pl.BlockSpec(memory_space=pltpu.VMEM)
    H, D = first.shape
    return pl.pallas_call(
        functools.partial(finish_kernel, Z, R),
        out_shape=jax.ShapeDtypeStruct((2 * H, D), jnp.bfloat16),
        in_specs=[vm, vm],
        out_specs=vm,
        scratch_shapes=[
            pltpu.VMEM((Z, H, D), jnp.bfloat16),
            pltpu.VMEM((Z, H, D), jnp.bfloat16),
            pltpu.VMEM((Z, H, D), jnp.bfloat16),
            pltpu.VMEM((H, D), jnp.float32),
            pltpu.SemaphoreType.DMA((2, Z)),
            pltpu.SemaphoreType.DMA((2, Z)),
            pltpu.SemaphoreType.DMA((2,)),
            pltpu.SemaphoreType.DMA,
        ],
        compiler_params=pltpu.CompilerParams(
            collective_id=2, has_side_effects=True, vmem_limit_bytes=VMEM_LIMIT
        ),
    )(terms, first)


def columns_form(
    resid,
    queries,
    keys,
    values,
    lambdas,
    head_gain,
    out_weight,
    norm_gain,
    gate_weight,
    up_weight,
    down_weight,
):
    Z = lambdas.shape[0]
    R = lax.axis_size("sp") // Z
    T, D = resid.shape
    share = gate_weight.shape[1] // Z
    q, k, v, g, u, d = gather_all(Z, R, queries, keys, values, gate_weight, up_weight, down_weight)
    S = Z * R
    ho = attention(
        Z, R, q, k.reshape(S * T, VD), v.reshape(S * T, VD), lambdas, head_gain
    )
    first, normed = branch(Z, R, ho, resid, out_weight, norm_gain)
    width = g.shape[2]
    gate = jnp.dot(normed, g.reshape(D, width), preferred_element_type=jnp.float32)
    up = jnp.dot(normed, u.reshape(D, width), preferred_element_type=jnp.float32)
    z = lax.axis_index("sp") // R
    unit = first_block(z, share) * LANE + lax.iota(jnp.int32, width)
    counted = (unit >= z * share) & (unit < (z + 1) * share)
    hidden = jnp.where(counted[None, :], jax.nn.silu(gate) * up, 0.0).astype(jnp.bfloat16)
    terms = jnp.dot(
        hidden, jnp.transpose(d, (1, 0, 2)).reshape(width, D), preferred_element_type=jnp.float32
    ).astype(jnp.bfloat16)
    return finish(Z, R, terms.reshape(Z, 2, T // 2, D), first)


def solution(mesh):
    sp, tp = mesh.shape["sp"], mesh.shape["tp"]

    def local(*args):
        heads = args[4].shape[0]
        tok_rows = args[1].shape[0]
        columns = (
            tp == 2
            and heads > 1
            and sp == 4 * heads
            and args[10].shape[1] % LANE == 0
            and args[8].shape[1] % (16 * heads) == 0
            and tok_rows % 32 == 0
        )
        return (columns_form if columns else generic)(*args)

    return jax.shard_map(
        local,
        mesh=mesh,
        in_specs=(
            P("sp", None),
            P("sp", "tp"),
            P("sp", "tp"),
            P("sp", "tp"),
            P("tp"),
            P(),
            P("tp", None),
            P(),
            P("sp", "tp"),
            P("sp", "tp"),
            P("tp", "sp"),
        ),
        out_specs=P("sp", None),
        check_vma=False,
    )
```

```python
import jax
import jax.numpy as jnp
from jax import lax
from jax.experimental import pallas as pl
from jax.experimental.pallas import tpu as pltpu
from jax.sharding import PartitionSpec as P

QK = 64
VD = 128
LANE = 128
VMEM_LIMIT = 60 * 1024 * 1024


def rms_rows(first, norm_gain):
    return (
        first * lax.rsqrt(jnp.mean(first * first, axis=-1, keepdims=True) + 1e-06) * norm_gain
    ).astype(jnp.bfloat16)


def generic(
    resid,
    queries,
    keys,
    values,
    lambdas,
    head_gain,
    out_weight,
    norm_gain,
    gate_weight,
    up_weight,
    down_weight,
):
    tok_rows = queries.shape[0]
    local_heads = lambdas.shape[0]
    model_width = resid.shape[1]
    offset = lax.axis_index("sp") * tok_rows
    query_four = queries.reshape(tok_rows, local_heads, 2, QK)
    score_scale = QK ** (-0.5)
    query_pos = offset + lax.iota(jnp.int32, tok_rows)

    def update(fold_state, key_part, value_part, key_pos):
        run_max, run_sum, run_acc = fold_state
        scores = (
            jnp.einsum("qhcd,khcd->chqk", query_four, key_part, preferred_element_type=jnp.float32)
            * score_scale
        )
        causal_mask = key_pos[None, :] <= query_pos[:, None]
        scores = jnp.where(causal_mask, scores, -1e30)
        new_max = jnp.maximum(run_max, jnp.max(scores, axis=-1))
        expo = jnp.where(causal_mask, jnp.exp(scores - new_max[..., None]), 0.0)
        factor = jnp.exp(run_max - new_max)
        new_sum = run_sum * factor + jnp.sum(expo, axis=-1)
        new_acc = run_acc * factor[..., None] + jnp.einsum(
            "chqk,khd->chqd",
            expo.astype(jnp.bfloat16),
            value_part,
            preferred_element_type=jnp.float32,
        )
        return (new_max, new_sum, new_acc)

    initial = (
        jnp.full((2, local_heads, tok_rows), -1e30, jnp.float32),
        jnp.zeros((2, local_heads, tok_rows), jnp.float32),
        jnp.zeros((2, local_heads, tok_rows, VD), jnp.float32),
    )
    key_rows = lax.all_gather(keys, "sp", axis=0, tiled=True)
    value_rows = lax.all_gather(values, "sp", axis=0, tiled=True)
    key_count = key_rows.shape[0]
    key_span = key_count
    while key_span > 1024 and key_span % 2 == 0:
        key_span = key_span // 2

    def one_span(span_index, inner_state):
        span_start = span_index * key_span
        key_part = lax.dynamic_slice_in_dim(key_rows, span_start, key_span, 0).reshape(
            key_span, local_heads, 2, QK
        )
        value_part = lax.dynamic_slice_in_dim(value_rows, span_start, key_span, 0).reshape(
            key_span, local_heads, VD
        )
        key_pos = span_start + lax.iota(jnp.int32, key_span)
        return update(inner_state, key_part, value_part, key_pos)

    final_max, final_sum, final_acc = lax.fori_loop(0, key_count // key_span, one_span, initial)
    ratio = final_acc / final_sum[..., None]
    mixed_heads = ratio[0] - lambdas[:, None, None] * ratio[1]
    head_out = (
        mixed_heads
        * lax.rsqrt(jnp.mean(mixed_heads * mixed_heads, axis=-1, keepdims=True) + 1e-05)
        * head_gain
    ).astype(jnp.bfloat16)
    out_three = out_weight.reshape(local_heads, VD, model_width)
    own_count = tok_rows // lax.axis_size("tp")
    branch = lax.psum_scatter(
        jnp.einsum("hqd,hde->qe", head_out, out_three, preferred_element_type=jnp.float32).astype(
            jnp.bfloat16
        ),
        "tp",
        scatter_dimension=0,
        tiled=True,
    ).astype(jnp.float32)
    resid_own = lax.dynamic_slice_in_dim(resid, lax.axis_index("tp") * own_count, own_count, 0)
    first = resid_own.astype(jnp.float32) + branch
    normed_all = lax.all_gather(rms_rows(first, norm_gain), "tp", axis=0, tiled=True)
    gate_act = jnp.dot(
        normed_all,
        lax.all_gather(gate_weight, "sp", axis=0, tiled=True),
        preferred_element_type=jnp.float32,
    )
    up_act = jnp.dot(
        normed_all,
        lax.all_gather(up_weight, "sp", axis=0, tiled=True),
        preferred_element_type=jnp.float32,
    )
    hidden = (jax.nn.silu(gate_act) * up_act).astype(jnp.bfloat16)
    terms = jnp.dot(
        hidden,
        lax.all_gather(down_weight, "sp", axis=1, tiled=True),
        preferred_element_type=jnp.float32,
    )
    mixer = lax.psum_scatter(
        terms.astype(jnp.bfloat16), "tp", scatter_dimension=0, tiled=True
    ).astype(jnp.float32)
    finished = (first + 0.5 * mixer).astype(jnp.bfloat16)
    return lax.all_gather(finished, "tp", axis=0, tiled=True)


def where_am_i(R):
    s = lax.axis_index("sp")
    return s // R, lax.rem(s, R), lax.axis_index("tp")


def remote(src, dst, send, recv, sp, tp):
    return pltpu.make_async_remote_copy(
        src_ref=src,
        dst_ref=dst,
        send_sem=send,
        recv_sem=recv,
        device_id={"sp": sp, "tp": tp},
        device_id_type=pl.DeviceIdType.MESH,
    )


def greet(peers):
    barrier = pltpu.get_barrier_semaphore()
    for sp, tp in peers:
        pl.semaphore_signal(
            barrier,
            inc=1,
            device_id={"sp": sp, "tp": tp},
            device_id_type=pl.DeviceIdType.MESH,
        )
    pl.semaphore_wait(barrier, len(peers))


def first_block(zz, share):
    return (zz * share) // LANE


def mirror_x(r):
    return r + 1 - 2 * lax.rem(r, 2)


def mirror_y(r):
    return r + 2 - 4 * (lax.rem(r, 4) // 2)


def attention_block(R, T, i, r, q_at, k_at, v_at, lam, gain):
    span = R * T
    query = q_at(i) * jnp.bfloat16(QK**-0.5)
    ratios = []
    for c in range(2):
        part = query[:, c * QK : (c + 1) * QK]

        def fold(n, state, masked):
            run_max, run_sum, run_acc = state
            key = k_at(n)[:, c * QK : (c + 1) * QK]
            scores = lax.dot_general(
                part, key, (((1,), (1,)), ((), ())), preferred_element_type=jnp.float32
            )
            if masked:
                qpos = r * T + lax.broadcasted_iota(jnp.int32, scores.shape, 0)
                kpos = lax.broadcasted_iota(jnp.int32, scores.shape, 1)
                scores = jnp.where(kpos <= qpos, scores, -1e30)
            new_max = jnp.maximum(run_max, jnp.max(scores, axis=-1, keepdims=True))
            expo = jnp.exp(scores - new_max)
            factor = jnp.exp(run_max - new_max)
            new_sum = run_sum * factor + jnp.sum(expo, axis=-1, keepdims=True)
            new_acc = run_acc * factor + jnp.dot(
                expo.astype(jnp.bfloat16), v_at(n), preferred_element_type=jnp.float32
            )
            return new_max, new_sum, new_acc

        state = (
            jnp.full((T, 1), -1e30, jnp.float32),
            jnp.zeros((T, 1), jnp.float32),
            jnp.zeros((T, VD), jnp.float32),
        )
        state = fold(i, state, True)
        state = lax.fori_loop(0, i, lambda n, st: fold(n, st, False), state)
        ratios.append(state[2] / state[1])
    mixed = ratios[0] - lam * ratios[1]
    return (
        mixed * lax.rsqrt(jnp.mean(mixed * mixed, axis=-1, keepdims=True) + 1e-05) * gain
    ).astype(jnp.bfloat16)


def whole_kernel(Z, R, share, width, refs):
    (
        q_in, k_in, v_in, g_in, u_in, d_in, resid_in, w_in, lam, head_gain, norm_gain,
        out,
        q_sc, k_sc, v_sc, g_sc, u_sc, d_sc, resid, w,
        ho, heads, part, got, first, norm_sc, all_sc,
        hidden, terms, cross, sums, landed,
        send1, recv1, send2, recv2, local_sem, ho_sem, swap_sem, ag_sem, core_sem,
        cross_sem, sum_sem, out_sem,
    ) = refs
    ins = (q_in, k_in, v_in, g_in, u_in, d_in)
    outs = (q_sc, k_sc, v_sc, g_sc, u_sc, d_sc)
    z, r, t = where_am_i(R)
    me = z * R + r
    rx, ry = mirror_x(r), mirror_y(r)
    rd = mirror_x(ry)
    T = k_in.shape[0]
    W = g_in.shape[0]
    D = resid_in.shape[1]
    H = T // 2
    ahead = [lax.rem(z + j, Z) for j in range(Z)]
    behind = [lax.rem(z + Z - j, Z) for j in range(Z)]

    def dev(zz, rr):
        return zz * R + rr

    greet(
        [(dev(ahead[j], r), t) for j in range(1, Z)]
        + [(dev(z, rx), t), (dev(z, ry), t), (me, 1 - t)]
    )

    def source(a, zz, h=None):
        ref = ins[a]
        if a == 5:
            start = pl.multiple_of(first_block(zz, share) * LANE, LANE)
            if h is None:
                return ref.at[pl.ds(start, width), :]
            n = width // 2
            return ref.at[pl.ds(pl.multiple_of(start + h * n, 64), n), :]
        if a < 3:
            rows, sl = T, pl.ds(pl.multiple_of(zz * VD, LANE), VD)
        else:
            rows, sl = W, pl.ds(pl.multiple_of(first_block(zz, share) * LANE, LANE), width)
        if h is None:
            return ref.at[:, sl]
        n = rows // 2
        return ref.at[pl.ds(h * n, n), sl]

    def place(a, zz, rr, h=None):
        ref = outs[a]
        if a == 0:
            return ref.at[zz]
        slot = dev(zz, rr)
        if h is None:
            return ref.at[slot]
        n = ref.shape[1] // 2
        return ref.at[slot, pl.ds(h * n, n), :]

    started, locals_ = [], []

    def first_hop(a, j):
        c = remote(
            source(a, ahead[j]), place(a, z, r), send1.at[a, j], recv1.at[a, j], dev(ahead[j], r), t
        )
        c.start()
        started.append(c)

    def arrived(a, j):
        zz = behind[j]
        remote(
            source(a, z), place(a, zz, r), send1.at[a, j], recv1.at[a, j], dev(zz, r), t
        ).wait_recv()

    def keep(src, dst, n):
        c = pltpu.make_async_copy(src, dst, local_sem.at[n])
        c.start()
        locals_.append(c)

    def hop2(a, j, kind, owner, h, target, from_input):
        zz = behind[j]
        src = source(a, z, h) if from_input else place(a, zz, owner, h)
        return remote(
            src,
            place(a, zz, owner, h),
            send2.at[a - 1, j, kind],
            recv2.at[a - 1, j, kind],
            dev(z, target),
            t,
        )

    def wait2(a, j, kind):
        owner = (rx, rx, ry, ry, rd, rd)[kind]
        target = (rx, rx, ry, ry, ry, rx)[kind]
        hop2(a, j, kind, owner, kind % 2, target, False).wait_recv()

    def send_piece(a, j):
        if j:
            arrived(a, j)
        for kind, h, target in ((0, 0, rx), (3, 1, ry), (1, 1, rx), (2, 0, ry)):
            c = hop2(a, j, kind, r, h, target, j == 0)
            c.start()
            started.append(c)

    def forward_piece(a, j):
        wait2(a, j, 0)
        c = hop2(a, j, 4, rx, 0, ry, False)
        c.start()
        started.append(c)
        wait2(a, j, 3)
        c = hop2(a, j, 5, ry, 1, rx, False)
        c.start()
        started.append(c)

    small = [(a, j) for j in range(Z) for a in (1, 2)]
    for j in range(1, Z):
        for a in (1, 2, 0):
            first_hop(a, j)
    for a in (1, 2):
        send_piece(a, 0)
    for a in (3, 4, 5):
        first_hop(a, 1)
    for a in range(6):
        keep(source(a, z), place(a, z, r), a)
    keep(resid_in, resid, 6)
    keep(w_in, w, 7)
    lag = 2
    for i in range(2, len(small) + lag):
        if i < len(small):
            send_piece(*small[i])
        if i == len(small) - 1:
            for a in (3, 4, 5):
                send_piece(a, 0)
        forward_piece(*small[i - lag])
    for j in range(2, Z - 1):
        for a in (3, 4, 5):
            first_hop(a, j)
    for a, j in small:
        for kind in (1, 2, 4, 5):
            wait2(a, j, kind)
    for j in range(1, Z):
        arrived(0, j)
    for c in locals_:
        c.wait()

    head_lam = lam[z]

    def span(ref, n):
        return ref[pl.ds(n * R, R)].reshape(R * T, VD)

    @pl.loop(0, Z)
    def _(i):
        ho[i] = attention_block(
            R,
            T,
            i,
            r,
            lambda b: q_sc[b],
            lambda n: span(k_sc, n),
            lambda n: span(v_sc, n),
            head_lam,
            head_gain[...],
        )

    copies = []
    for j in range(1, Z):
        c = remote(
            ho.at[ahead[j]], heads.at[z], ho_sem.at[0, j], ho_sem.at[1, j], dev(ahead[j], r), t
        )
        c.start()
        copies.append(c)
    for a in (3, 4, 5):
        first_hop(a, Z - 1)
    heads[z] = ho[z]

    big = [(a, j) for j in range(Z) for a in (3, 4, 5)]
    big_lag = 3

    def service(i):
        if 3 <= i < len(big):
            send_piece(*big[i])
        if big_lag <= i < len(big) + big_lag:
            forward_piece(*big[i - big_lag])

    for i in range(3, 6):
        service(i)

    for c in copies:
        c.wait()
    NT = 512 if D % 512 == 0 else D
    for h in range(2):
        hh = (1 - t) if h == 0 else t
        rows = pl.ds(pl.multiple_of(hh * H, 16), H)
        left = jnp.concatenate([heads[n, rows, :] for n in range(Z)], axis=1)
        for n in range(0, D, NT):
            part[h, :, n : n + NT] = jnp.dot(
                left, w[:, n : n + NT], preferred_element_type=jnp.float32
            ).astype(jnp.bfloat16)
        if h == 0:
            swap = remote(part.at[0], got, swap_sem.at[0], swap_sem.at[1], me, 1 - t)
            swap.start()
    swap.wait()
    own_rows = pl.ds(pl.multiple_of(t * H, 16), H)
    first_val = resid[own_rows, :].astype(jnp.float32) + (
        part[1].astype(jnp.float32) + got[...].astype(jnp.float32)
    )
    first[...] = first_val
    norm_sc[...] = rms_rows(first_val, norm_gain[...])

    def rows_of(zz, tt):
        return all_sc.at[zz, tt]

    copies = []
    for j in range(1, Z):
        c = remote(
            norm_sc, rows_of(z, t), ag_sem.at[0, j], ag_sem.at[1, j], dev(ahead[j], r), t
        )
        c.start()
        copies.append(c)
    across = [remote(norm_sc, rows_of(z, t), core_sem.at[0, 0], core_sem.at[1, 0], me, 1 - t)]
    across[0].start()
    own = pltpu.make_async_copy(norm_sc, rows_of(z, t), local_sem.at[0])
    own.start()

    for i in range(6, len(big) + big_lag):
        service(i)

    for j in range(1, Z):
        zz = behind[j]
        remote(
            norm_sc, rows_of(zz, t), ag_sem.at[0, j], ag_sem.at[1, j], dev(zz, r), t
        ).wait_recv()
        c = remote(rows_of(zz, t), rows_of(zz, t), core_sem.at[0, j], core_sem.at[1, j], me, 1 - t)
        c.start()
        across.append(c)
    own.wait()
    for a, j in big:
        for kind in (1, 2, 4, 5):
            wait2(a, j, kind)
    for j in range(Z):
        zz = behind[j]
        remote(
            rows_of(zz, t), rows_of(zz, 1 - t), core_sem.at[0, j], core_sem.at[1, j], me, 1 - t
        ).wait_recv()

    FT = 256 if width % 256 == 0 else LANE
    DN = d_sc.shape[2]
    low = first_block(z, share) * LANE
    sent = []
    order = [j % Z for j in range(1, Z + 1)]
    for n, j in enumerate(order):
        zz = ahead[j]
        block = all_sc[zz].reshape(T, D)

        @pl.loop(0, width // FT)
        def _(f, block=block):
            cols = pl.ds(pl.multiple_of(f * FT, FT), FT)
            gate = jnp.dot(
                block, g_sc[:, :, cols].reshape(D, FT), preferred_element_type=jnp.float32
            )
            up = jnp.dot(
                block, u_sc[:, :, cols].reshape(D, FT), preferred_element_type=jnp.float32
            )
            unit = low + f * FT + lax.broadcasted_iota(jnp.int32, gate.shape, 1)
            counted = (unit >= z * share) & (unit < (z + 1) * share)
            value = jax.nn.silu(gate) * up
            hidden[:, cols] = jnp.where(counted, value, 0.0).astype(jnp.bfloat16)

        left = hidden[...]

        @pl.loop(0, (Z * R) // 2)
        def _(p, left=left, n=n):
            right = jnp.concatenate([d_sc[2 * p], d_sc[2 * p + 1]], axis=1)
            value = jnp.dot(left, right, preferred_element_type=jnp.float32).astype(jnp.bfloat16)
            cols = pl.ds(pl.multiple_of(p * (2 * DN), 2 * DN), 2 * DN)
            terms[n, :, :, cols] = value.reshape(2, H, 2 * DN)

        c = remote(
            terms.at[n, 1 - t], cross.at[n], cross_sem.at[0, n], cross_sem.at[1, n], me, 1 - t
        )
        c.start()
        c.wait()
        total = terms[n, t].astype(jnp.float32) + cross[n].astype(jnp.float32)
        if j:
            sums[j] = total.astype(jnp.bfloat16)
            c = remote(
                sums.at[j], landed.at[j], sum_sem.at[0, j], sum_sem.at[1, j], dev(zz, r), t
            )
            c.start()
            sent.append(c)
        else:
            first[...] = first[...] + 0.5 * total
    for c in sent:
        c.wait()
    total = landed[1].astype(jnp.float32)
    for j in range(2, Z):
        total = total + landed[j].astype(jnp.float32)
    sums[0] = (first[...] + 0.5 * total).astype(jnp.bfloat16)
    c = remote(sums.at[0], out.at[own_rows, :], out_sem.at[0], out_sem.at[1], me, 1 - t)
    c.start()
    own = pltpu.make_async_copy(sums.at[0], out.at[own_rows, :], local_sem.at[1])
    own.start()
    own.wait()
    c.wait()
    for c in started + copies + across:
        c.wait_send()


def columns_form(
    resid,
    queries,
    keys,
    values,
    lambdas,
    head_gain,
    out_weight,
    norm_gain,
    gate_weight,
    up_weight,
    down_weight,
):
    Z = lambdas.shape[0]
    S = lax.axis_size("sp")
    R = S // Z
    T, D = resid.shape
    H = T // 2
    W = gate_weight.shape[0]
    DN = down_weight.shape[1]
    share = gate_weight.shape[1] // Z
    width = LANE * max(
        -(-((zz + 1) * share) // LANE) - (zz * share) // LANE for zz in range(Z)
    )
    bf, f32 = jnp.bfloat16, jnp.float32
    vm = pl.BlockSpec(memory_space=pltpu.VMEM)
    hbm = pl.BlockSpec(memory_space=pl.ANY)
    dma = pltpu.SemaphoreType.DMA

    def kernel(*refs):
        whole_kernel(Z, R, share, width, refs)

    return pl.pallas_call(
        kernel,
        out_shape=jax.ShapeDtypeStruct((T, D), bf),
        in_specs=[hbm] * 8 + [pl.BlockSpec(memory_space=pltpu.SMEM), vm, vm],
        out_specs=vm,
        scratch_shapes=[
            pltpu.VMEM((Z, T, VD), bf),
            pltpu.VMEM((S, T, VD), bf),
            pltpu.VMEM((S, T, VD), bf),
            pltpu.VMEM((S, W, width), bf),
            pltpu.VMEM((S, W, width), bf),
            pltpu.VMEM((S, width, DN), bf),
            pltpu.VMEM((T, D), bf),
            pltpu.VMEM(out_weight.shape, bf),
            pltpu.VMEM((Z, T, VD), bf),
            pltpu.VMEM((Z, T, VD), bf),
            pltpu.VMEM((2, H, D), bf),
            pltpu.VMEM((H, D), bf),
            pltpu.VMEM((H, D), f32),
            pltpu.VMEM((H, D), bf),
            pltpu.VMEM((Z, 2, H, D), bf),
            pltpu.VMEM((T, width), bf),
            pltpu.VMEM((Z, 2, H, D), bf),
            pltpu.VMEM((Z, H, D), bf),
            pltpu.VMEM((Z, H, D), bf),
            pltpu.VMEM((Z, H, D), bf),
            dma((6, Z)),
            dma((6, Z)),
            dma((5, Z, 6)),
            dma((5, Z, 6)),
            dma((8,)),
            dma((2, Z)),
            dma((2,)),
            dma((2, Z)),
            dma((2, Z)),
            dma((2, Z)),
            dma((2, Z)),
            dma((2,)),
        ],
        compiler_params=pltpu.CompilerParams(
            collective_id=0, has_side_effects=True, vmem_limit_bytes=VMEM_LIMIT
        ),
    )(
        queries,
        keys,
        values,
        gate_weight,
        up_weight,
        down_weight,
        resid,
        out_weight,
        lambdas,
        head_gain.reshape(1, -1),
        norm_gain.reshape(1, -1),
    )


def solution(mesh):
    sp, tp = mesh.shape["sp"], mesh.shape["tp"]

    def local(*args):
        heads = args[4].shape[0]
        tok_rows = args[1].shape[0]
        columns = (
            tp == 2
            and heads > 2
            and sp == 4 * heads
            and args[10].shape[1] % LANE == 0
            and args[8].shape[1] % (16 * heads) == 0
            and tok_rows % 32 == 0
        )
        return (columns_form if columns else generic)(*args)

    return jax.shard_map(
        local,
        mesh=mesh,
        in_specs=(
            P("sp", None),
            P("sp", "tp"),
            P("sp", "tp"),
            P("sp", "tp"),
            P("tp"),
            P(),
            P("tp", None),
            P(),
            P("sp", "tp"),
            P("sp", "tp"),
            P("tp", "sp"),
        ),
        out_specs=P("sp", None),
        check_vma=False,
    )
```

```python
import jax
import jax.numpy as jnp
from jax import lax
from jax.experimental import pallas as pl
from jax.experimental.pallas import tpu as pltpu
from jax.sharding import PartitionSpec as P

QK = 64
VD = 128
LANE = 128
VMEM_LIMIT = 60 * 1024 * 1024


def rms_rows(first, norm_gain):
    return (
        first * lax.rsqrt(jnp.mean(first * first, axis=-1, keepdims=True) + 1e-06) * norm_gain
    ).astype(jnp.bfloat16)


def generic(
    resid,
    queries,
    keys,
    values,
    lambdas,
    head_gain,
    out_weight,
    norm_gain,
    gate_weight,
    up_weight,
    down_weight,
):
    tok_rows = queries.shape[0]
    local_heads = lambdas.shape[0]
    model_width = resid.shape[1]
    offset = lax.axis_index("sp") * tok_rows
    query_four = queries.reshape(tok_rows, local_heads, 2, QK)
    score_scale = QK ** (-0.5)
    query_pos = offset + lax.iota(jnp.int32, tok_rows)

    def update(fold_state, key_part, value_part, key_pos):
        run_max, run_sum, run_acc = fold_state
        scores = (
            jnp.einsum("qhcd,khcd->chqk", query_four, key_part, preferred_element_type=jnp.float32)
            * score_scale
        )
        causal_mask = key_pos[None, :] <= query_pos[:, None]
        scores = jnp.where(causal_mask, scores, -1e30)
        new_max = jnp.maximum(run_max, jnp.max(scores, axis=-1))
        expo = jnp.where(causal_mask, jnp.exp(scores - new_max[..., None]), 0.0)
        factor = jnp.exp(run_max - new_max)
        new_sum = run_sum * factor + jnp.sum(expo, axis=-1)
        new_acc = run_acc * factor[..., None] + jnp.einsum(
            "chqk,khd->chqd",
            expo.astype(jnp.bfloat16),
            value_part,
            preferred_element_type=jnp.float32,
        )
        return (new_max, new_sum, new_acc)

    initial = (
        jnp.full((2, local_heads, tok_rows), -1e30, jnp.float32),
        jnp.zeros((2, local_heads, tok_rows), jnp.float32),
        jnp.zeros((2, local_heads, tok_rows, VD), jnp.float32),
    )
    key_rows = lax.all_gather(keys, "sp", axis=0, tiled=True)
    value_rows = lax.all_gather(values, "sp", axis=0, tiled=True)
    key_count = key_rows.shape[0]
    key_span = key_count
    while key_span > 1024 and key_span % 2 == 0:
        key_span = key_span // 2

    def one_span(span_index, inner_state):
        span_start = span_index * key_span
        key_part = lax.dynamic_slice_in_dim(key_rows, span_start, key_span, 0).reshape(
            key_span, local_heads, 2, QK
        )
        value_part = lax.dynamic_slice_in_dim(value_rows, span_start, key_span, 0).reshape(
            key_span, local_heads, VD
        )
        key_pos = span_start + lax.iota(jnp.int32, key_span)
        return update(inner_state, key_part, value_part, key_pos)

    final_max, final_sum, final_acc = lax.fori_loop(0, key_count // key_span, one_span, initial)
    ratio = final_acc / final_sum[..., None]
    mixed_heads = ratio[0] - lambdas[:, None, None] * ratio[1]
    head_out = (
        mixed_heads
        * lax.rsqrt(jnp.mean(mixed_heads * mixed_heads, axis=-1, keepdims=True) + 1e-05)
        * head_gain
    ).astype(jnp.bfloat16)
    out_three = out_weight.reshape(local_heads, VD, model_width)
    own_count = tok_rows // lax.axis_size("tp")
    branch = lax.psum_scatter(
        jnp.einsum("hqd,hde->qe", head_out, out_three, preferred_element_type=jnp.float32).astype(
            jnp.bfloat16
        ),
        "tp",
        scatter_dimension=0,
        tiled=True,
    ).astype(jnp.float32)
    resid_own = lax.dynamic_slice_in_dim(resid, lax.axis_index("tp") * own_count, own_count, 0)
    first = resid_own.astype(jnp.float32) + branch
    normed_all = lax.all_gather(rms_rows(first, norm_gain), "tp", axis=0, tiled=True)
    gate_act = jnp.dot(
        normed_all,
        lax.all_gather(gate_weight, "sp", axis=0, tiled=True),
        preferred_element_type=jnp.float32,
    )
    up_act = jnp.dot(
        normed_all,
        lax.all_gather(up_weight, "sp", axis=0, tiled=True),
        preferred_element_type=jnp.float32,
    )
    hidden = (jax.nn.silu(gate_act) * up_act).astype(jnp.bfloat16)
    terms = jnp.dot(
        hidden,
        lax.all_gather(down_weight, "sp", axis=1, tiled=True),
        preferred_element_type=jnp.float32,
    )
    mixer = lax.psum_scatter(
        terms.astype(jnp.bfloat16), "tp", scatter_dimension=0, tiled=True
    ).astype(jnp.float32)
    finished = (first + 0.5 * mixer).astype(jnp.bfloat16)
    return lax.all_gather(finished, "tp", axis=0, tiled=True)


def where_am_i(R):
    s = lax.axis_index("sp")
    return s // R, lax.rem(s, R), lax.axis_index("tp")


def remote(src, dst, send, recv, sp, tp):
    return pltpu.make_async_remote_copy(
        src_ref=src,
        dst_ref=dst,
        send_sem=send,
        recv_sem=recv,
        device_id={"sp": sp, "tp": tp},
        device_id_type=pl.DeviceIdType.MESH,
    )


def greet(peers):
    barrier = pltpu.get_barrier_semaphore()
    for sp, tp in peers:
        pl.semaphore_signal(
            barrier,
            inc=1,
            device_id={"sp": sp, "tp": tp},
            device_id_type=pl.DeviceIdType.MESH,
        )
    pl.semaphore_wait(barrier, len(peers))


def first_block(zz, share):
    return (zz * share) // LANE


def mirror_x(r):
    return r + 1 - 2 * lax.rem(r, 2)


def mirror_y(r):
    return r + 2 - 4 * (lax.rem(r, 4) // 2)


def attention_block(R, T, i, r, q_at, k_at, v_at, lam, gain):
    span = R * T
    query = q_at(i) * jnp.bfloat16(QK**-0.5)
    ratios = []
    for c in range(2):
        part = query[:, c * QK : (c + 1) * QK]

        def fold(n, state, masked):
            run_max, run_sum, run_acc = state
            key = k_at(n)[:, c * QK : (c + 1) * QK]
            scores = lax.dot_general(
                part, key, (((1,), (1,)), ((), ())), preferred_element_type=jnp.float32
            )
            if masked:
                qpos = r * T + lax.broadcasted_iota(jnp.int32, scores.shape, 0)
                kpos = lax.broadcasted_iota(jnp.int32, scores.shape, 1)
                scores = jnp.where(kpos <= qpos, scores, -1e30)
            new_max = jnp.maximum(run_max, jnp.max(scores, axis=-1, keepdims=True))
            expo = jnp.exp(scores - new_max)
            factor = jnp.exp(run_max - new_max)
            new_sum = run_sum * factor + jnp.sum(expo, axis=-1, keepdims=True)
            new_acc = run_acc * factor + jnp.dot(
                expo.astype(jnp.bfloat16), v_at(n), preferred_element_type=jnp.float32
            )
            return new_max, new_sum, new_acc

        state = (
            jnp.full((T, 1), -1e30, jnp.float32),
            jnp.zeros((T, 1), jnp.float32),
            jnp.zeros((T, VD), jnp.float32),
        )
        state = fold(i, state, True)
        state = lax.fori_loop(0, i, lambda n, st: fold(n, st, False), state)
        ratios.append(state[2] / state[1])
    mixed = ratios[0] - lam * ratios[1]
    return (
        mixed * lax.rsqrt(jnp.mean(mixed * mixed, axis=-1, keepdims=True) + 1e-05) * gain
    ).astype(jnp.bfloat16)


def whole_kernel(Z, R, share, width, refs):
    (
        q_in, k_in, v_in, g_in, u_in, d_in, resid_in, w_in, lam, head_gain, norm_gain,
        out,
        q_sc, k_sc, v_sc, g_sc, u_sc, d_sc, resid, w,
        ho, heads, part, got, first, norm_sc, all_sc,
        hidden, terms, cross, sums, landed,
        send1, recv1, send2, recv2, local_sem, ho_sem, swap_sem, ag_sem, core_sem,
        cross_sem, sum_sem, out_sem,
    ) = refs
    ins = (q_in, k_in, v_in, g_in, u_in, d_in)
    outs = (q_sc, k_sc, v_sc, g_sc, u_sc, d_sc)
    z, r, t = where_am_i(R)
    me = z * R + r
    rx, ry = mirror_x(r), mirror_y(r)
    rd = mirror_x(ry)
    T = k_in.shape[0]
    W = g_in.shape[0]
    D = resid_in.shape[1]
    H = T // 2
    ahead = [lax.rem(z + j, Z) for j in range(Z)]
    behind = [lax.rem(z + Z - j, Z) for j in range(Z)]

    def dev(zz, rr):
        return zz * R + rr

    greet(
        [(dev(ahead[j], r), t) for j in range(1, Z)]
        + [(dev(z, rx), t), (dev(z, ry), t), (me, 1 - t)]
    )

    def source(a, zz, h=None):
        ref = ins[a]
        if a == 5:
            start = pl.multiple_of(first_block(zz, share) * LANE, LANE)
            if h is None:
                return ref.at[pl.ds(start, width), :]
            n = width // 2
            return ref.at[pl.ds(pl.multiple_of(start + h * n, 64), n), :]
        if a < 3:
            rows, sl = T, pl.ds(pl.multiple_of(zz * VD, LANE), VD)
        else:
            rows, sl = W, pl.ds(pl.multiple_of(first_block(zz, share) * LANE, LANE), width)
        if h is None:
            return ref.at[:, sl]
        n = rows // 2
        return ref.at[pl.ds(h * n, n), sl]

    def place(a, zz, rr, h=None):
        ref = outs[a]
        if a == 0:
            return ref.at[zz]
        slot = dev(zz, rr)
        if h is None:
            return ref.at[slot]
        n = ref.shape[1] // 2
        return ref.at[slot, pl.ds(h * n, n), :]

    started, locals_ = [], []

    def first_hop(a, j):
        c = remote(
            source(a, ahead[j]), place(a, z, r), send1.at[a, j], recv1.at[a, j], dev(ahead[j], r), t
        )
        c.start()
        started.append(c)

    def arrived(a, j):
        zz = behind[j]
        remote(
            source(a, z), place(a, zz, r), send1.at[a, j], recv1.at[a, j], dev(zz, r), t
        ).wait_recv()

    def keep(src, dst, n):
        c = pltpu.make_async_copy(src, dst, local_sem.at[n])
        c.start()
        locals_.append(c)

    def hop2(a, j, kind, owner, h, target, from_input):
        zz = behind[j]
        src = source(a, z, h) if from_input else place(a, zz, owner, h)
        return remote(
            src,
            place(a, zz, owner, h),
            send2.at[a - 1, j, kind],
            recv2.at[a - 1, j, kind],
            dev(z, target),
            t,
        )

    def wait2(a, j, kind):
        owner = (rx, rx, ry, ry, rd, rd)[kind]
        target = (rx, rx, ry, ry, ry, rx)[kind]
        hop2(a, j, kind, owner, kind % 2, target, False).wait_recv()

    def send_piece(a, j):
        if j:
            arrived(a, j)
        for kind, h, target in ((0, 0, rx), (3, 1, ry), (1, 1, rx), (2, 0, ry)):
            c = hop2(a, j, kind, r, h, target, j == 0)
            c.start()
            started.append(c)

    def forward_piece(a, j):
        wait2(a, j, 0)
        c = hop2(a, j, 4, rx, 0, ry, False)
        c.start()
        started.append(c)
        wait2(a, j, 3)
        c = hop2(a, j, 5, ry, 1, rx, False)
        c.start()
        started.append(c)

    small = [(a, j) for j in range(Z) for a in (1, 2)]
    for j in range(1, Z):
        for a in (1, 2, 0):
            first_hop(a, j)
    for a in (1, 2):
        send_piece(a, 0)
    for a in (3, 4, 5):
        first_hop(a, 1)
    for j in range(2, Z - 1):
        for a in (3, 4):
            first_hop(a, j)
    for a in range(6):
        keep(source(a, z), place(a, z, r), a)
    keep(resid_in, resid, 6)
    keep(w_in, w, 7)
    lag = 2
    for i in range(2, len(small) + lag):
        if i in (2, 4, 6):
            send_piece(2 + i // 2, 0)
        if i < len(small):
            send_piece(*small[i])
        forward_piece(*small[i - lag])
    for j in range(2, Z - 1):
        first_hop(5, j)
    for a, j in small:
        for kind in (1, 2, 4, 5):
            wait2(a, j, kind)
    for j in range(1, Z):
        arrived(0, j)
    for c in locals_:
        c.wait()

    head_lam = lam[z]

    def span(ref, n):
        return ref[pl.ds(n * R, R)].reshape(R * T, VD)

    @pl.loop(0, Z)
    def _(i):
        ho[i] = attention_block(
            R,
            T,
            i,
            r,
            lambda b: q_sc[b],
            lambda n: span(k_sc, n),
            lambda n: span(v_sc, n),
            head_lam,
            head_gain[...],
        )

    copies = []
    for j in range(1, Z):
        c = remote(
            ho.at[ahead[j]], heads.at[z], ho_sem.at[0, j], ho_sem.at[1, j], dev(ahead[j], r), t
        )
        c.start()
        copies.append(c)
    for a in (3, 4, 5):
        first_hop(a, Z - 1)
    heads[z] = ho[z]

    big = [(a, j) for j in range(Z) for a in (3, 4, 5)]
    big_lag = 3

    def service(i):
        if 3 <= i < len(big):
            send_piece(*big[i])
        if big_lag <= i < len(big) + big_lag:
            forward_piece(*big[i - big_lag])

    for i in range(3, 6):
        service(i)

    for c in copies:
        c.wait()
    NT = 512 if D % 512 == 0 else D
    for h in range(2):
        hh = (1 - t) if h == 0 else t
        rows = pl.ds(pl.multiple_of(hh * H, 16), H)
        left = jnp.concatenate([heads[n, rows, :] for n in range(Z)], axis=1)
        for n in range(0, D, NT):
            part[h, :, n : n + NT] = jnp.dot(
                left, w[:, n : n + NT], preferred_element_type=jnp.float32
            ).astype(jnp.bfloat16)
        if h == 0:
            swap = remote(part.at[0], got, swap_sem.at[0], swap_sem.at[1], me, 1 - t)
            swap.start()
    swap.wait()
    own_rows = pl.ds(pl.multiple_of(t * H, 16), H)
    first_val = resid[own_rows, :].astype(jnp.float32) + (
        part[1].astype(jnp.float32) + got[...].astype(jnp.float32)
    )
    first[...] = first_val
    norm_sc[...] = rms_rows(first_val, norm_gain[...])

    def rows_of(zz, tt):
        return all_sc.at[zz, tt]

    def ag_hop(down, d):
        zz = z + (d - 1) if down else z - (d - 1)
        to = z - 1 if down else z + 1
        return remote(
            norm_sc if d == 1 else rows_of(zz, t),
            rows_of(zz, t),
            ag_sem.at[2 * down, d],
            ag_sem.at[2 * down + 1, d],
            dev(to, r),
            t,
        )

    def sends(down, d):
        return (z > 0) & (z + (d - 1) < Z) if down else (z + 1 < Z) & (z - (d - 1) >= 0)

    def gets(down, d):
        return z + d < Z if down else z - d >= 0

    def origin(down, d):
        return z + d if down else z - d

    def to_core(down, d, tt):
        rows = rows_of(origin(down, d), tt)
        n = 2 * d + down
        return remote(rows, rows, core_sem.at[0, n], core_sem.at[1, n], me, 1 - t)

    def ag_start(d):
        for down in (0, 1):

            @pl.when(sends(down, d))
            def _(down=down):
                ag_hop(down, d).start()

    def ag_step(d):
        for down in (0, 1):

            @pl.when(gets(down, d))
            def _(down=down):
                rows = rows_of(origin(down, d), t)
                remote(
                    rows, rows, ag_sem.at[2 * down, d], ag_sem.at[2 * down + 1, d], me, 1 - t
                ).wait_recv()
                if d < Z - 1:

                    @pl.when(sends(down, d + 1))
                    def _():
                        ag_hop(down, d + 1).start()

                to_core(down, d, t).start()

    ag_start(1)
    across = remote(norm_sc, rows_of(z, t), core_sem.at[0, 0], core_sem.at[1, 0], me, 1 - t)
    across.start()
    own = pltpu.make_async_copy(norm_sc, rows_of(z, t), local_sem.at[0])
    own.start()

    for i in range(6, len(big)):
        service(i)
    done = 1
    for i in range(len(big), len(big) + big_lag):
        if done < Z:
            ag_step(done)
            done += 1
        service(i)
    for d in range(done, Z):
        ag_step(d)
    own.wait()
    for a, j in big:
        for kind in (1, 2, 4, 5):
            wait2(a, j, kind)
    across.wait_send()
    remote(
        norm_sc, rows_of(z, 1 - t), core_sem.at[0, 0], core_sem.at[1, 0], me, 1 - t
    ).wait_recv()
    for d in range(1, Z):
        for down in (0, 1):

            @pl.when(gets(down, d))
            def _(down=down, d=d):
                to_core(down, d, 1 - t).wait_recv()
                to_core(down, d, t).wait_send()

            @pl.when(sends(down, d))
            def _(down=down, d=d):
                ag_hop(down, d).wait_send()

    FT = 256 if width % 256 == 0 else LANE
    DN = d_sc.shape[2]
    low = first_block(z, share) * LANE
    sent = []
    order = [j % Z for j in range(1, Z + 1)]
    for n, j in enumerate(order):
        zz = ahead[j]
        block = all_sc[zz].reshape(T, D)

        @pl.loop(0, width // FT)
        def _(f, block=block):
            cols = pl.ds(pl.multiple_of(f * FT, FT), FT)
            gate = jnp.dot(
                block, g_sc[:, :, cols].reshape(D, FT), preferred_element_type=jnp.float32
            )
            up = jnp.dot(
                block, u_sc[:, :, cols].reshape(D, FT), preferred_element_type=jnp.float32
            )
            unit = low + f * FT + lax.broadcasted_iota(jnp.int32, gate.shape, 1)
            counted = (unit >= z * share) & (unit < (z + 1) * share)
            value = jax.nn.silu(gate) * up
            hidden[:, cols] = jnp.where(counted, value, 0.0).astype(jnp.bfloat16)

        left = hidden[...]

        @pl.loop(0, (Z * R) // 2)
        def _(p, left=left, n=n):
            right = jnp.concatenate([d_sc[2 * p], d_sc[2 * p + 1]], axis=1)
            value = jnp.dot(left, right, preferred_element_type=jnp.float32).astype(jnp.bfloat16)
            cols = pl.ds(pl.multiple_of(p * (2 * DN), 2 * DN), 2 * DN)
            terms[n, :, :, cols] = value.reshape(2, H, 2 * DN)

        c = remote(
            terms.at[n, 1 - t], cross.at[n], cross_sem.at[0, n], cross_sem.at[1, n], me, 1 - t
        )
        c.start()
        c.wait()
        total = terms[n, t].astype(jnp.float32) + cross[n].astype(jnp.float32)
        if j:
            sums[j] = total.astype(jnp.bfloat16)
            c = remote(
                sums.at[j], landed.at[j], sum_sem.at[0, j], sum_sem.at[1, j], dev(zz, r), t
            )
            c.start()
            sent.append(c)
        else:
            first[...] = first[...] + 0.5 * total
    for c in sent:
        c.wait()
    total = landed[1].astype(jnp.float32)
    for j in range(2, Z):
        total = total + landed[j].astype(jnp.float32)
    sums[0] = (first[...] + 0.5 * total).astype(jnp.bfloat16)
    c = remote(sums.at[0], out.at[own_rows, :], out_sem.at[0], out_sem.at[1], me, 1 - t)
    c.start()
    own = pltpu.make_async_copy(sums.at[0], out.at[own_rows, :], local_sem.at[1])
    own.start()
    own.wait()
    c.wait()
    for c in started:
        c.wait_send()


def columns_form(
    resid,
    queries,
    keys,
    values,
    lambdas,
    head_gain,
    out_weight,
    norm_gain,
    gate_weight,
    up_weight,
    down_weight,
):
    Z = lambdas.shape[0]
    S = lax.axis_size("sp")
    R = S // Z
    T, D = resid.shape
    H = T // 2
    W = gate_weight.shape[0]
    DN = down_weight.shape[1]
    share = gate_weight.shape[1] // Z
    width = LANE * max(
        -(-((zz + 1) * share) // LANE) - (zz * share) // LANE for zz in range(Z)
    )
    bf, f32 = jnp.bfloat16, jnp.float32
    vm = pl.BlockSpec(memory_space=pltpu.VMEM)
    hbm = pl.BlockSpec(memory_space=pl.ANY)
    dma = pltpu.SemaphoreType.DMA

    def kernel(*refs):
        whole_kernel(Z, R, share, width, refs)

    return pl.pallas_call(
        kernel,
        out_shape=jax.ShapeDtypeStruct((T, D), bf),
        in_specs=[hbm] * 8 + [pl.BlockSpec(memory_space=pltpu.SMEM), vm, vm],
        out_specs=vm,
        scratch_shapes=[
            pltpu.VMEM((Z, T, VD), bf),
            pltpu.VMEM((S, T, VD), bf),
            pltpu.VMEM((S, T, VD), bf),
            pltpu.VMEM((S, W, width), bf),
            pltpu.VMEM((S, W, width), bf),
            pltpu.VMEM((S, width, DN), bf),
            pltpu.VMEM((T, D), bf),
            pltpu.VMEM(out_weight.shape, bf),
            pltpu.VMEM((Z, T, VD), bf),
            pltpu.VMEM((Z, T, VD), bf),
            pltpu.VMEM((2, H, D), bf),
            pltpu.VMEM((H, D), bf),
            pltpu.VMEM((H, D), f32),
            pltpu.VMEM((H, D), bf),
            pltpu.VMEM((Z, 2, H, D), bf),
            pltpu.VMEM((T, width), bf),
            pltpu.VMEM((Z, 2, H, D), bf),
            pltpu.VMEM((Z, H, D), bf),
            pltpu.VMEM((Z, H, D), bf),
            pltpu.VMEM((Z, H, D), bf),
            dma((6, Z)),
            dma((6, Z)),
            dma((5, Z, 6)),
            dma((5, Z, 6)),
            dma((8,)),
            dma((2, Z)),
            dma((2,)),
            dma((4, Z)),
            dma((2, 2 * Z)),
            dma((2, Z)),
            dma((2, Z)),
            dma((2,)),
        ],
        compiler_params=pltpu.CompilerParams(
            collective_id=0, has_side_effects=True, vmem_limit_bytes=VMEM_LIMIT
        ),
    )(
        queries,
        keys,
        values,
        gate_weight,
        up_weight,
        down_weight,
        resid,
        out_weight,
        lambdas,
        head_gain.reshape(1, -1),
        norm_gain.reshape(1, -1),
    )


def solution(mesh):
    sp, tp = mesh.shape["sp"], mesh.shape["tp"]

    def local(*args):
        heads = args[4].shape[0]
        tok_rows = args[1].shape[0]
        columns = (
            tp == 2
            and heads > 2
            and sp == 4 * heads
            and args[10].shape[1] % LANE == 0
            and args[8].shape[1] % (16 * heads) == 0
            and tok_rows % 32 == 0
        )
        return (columns_form if columns else generic)(*args)

    return jax.shard_map(
        local,
        mesh=mesh,
        in_specs=(
            P("sp", None),
            P("sp", "tp"),
            P("sp", "tp"),
            P("sp", "tp"),
            P("tp"),
            P(),
            P("tp", None),
            P(),
            P("sp", "tp"),
            P("sp", "tp"),
            P("tp", "sp"),
        ),
        out_specs=P("sp", None),
        check_vma=False,
    )
```

```python
import jax
import jax.numpy as jnp
from jax import lax
from jax.experimental import pallas as pl
from jax.experimental.pallas import tpu as pltpu
from jax.sharding import PartitionSpec as P

QK = 64
VD = 128
LANE = 128
LATE = 3
VMEM_LIMIT = 60 * 1024 * 1024


def rms_rows(first, norm_gain):
    return (
        first * lax.rsqrt(jnp.mean(first * first, axis=-1, keepdims=True) + 1e-06) * norm_gain
    ).astype(jnp.bfloat16)


def generic(
    resid,
    queries,
    keys,
    values,
    lambdas,
    head_gain,
    out_weight,
    norm_gain,
    gate_weight,
    up_weight,
    down_weight,
):
    tok_rows = queries.shape[0]
    local_heads = lambdas.shape[0]
    model_width = resid.shape[1]
    offset = lax.axis_index("sp") * tok_rows
    query_four = queries.reshape(tok_rows, local_heads, 2, QK)
    score_scale = QK ** (-0.5)
    query_pos = offset + lax.iota(jnp.int32, tok_rows)

    def update(fold_state, key_part, value_part, key_pos):
        run_max, run_sum, run_acc = fold_state
        scores = (
            jnp.einsum("qhcd,khcd->chqk", query_four, key_part, preferred_element_type=jnp.float32)
            * score_scale
        )
        causal_mask = key_pos[None, :] <= query_pos[:, None]
        scores = jnp.where(causal_mask, scores, -1e30)
        new_max = jnp.maximum(run_max, jnp.max(scores, axis=-1))
        expo = jnp.where(causal_mask, jnp.exp(scores - new_max[..., None]), 0.0)
        factor = jnp.exp(run_max - new_max)
        new_sum = run_sum * factor + jnp.sum(expo, axis=-1)
        new_acc = run_acc * factor[..., None] + jnp.einsum(
            "chqk,khd->chqd",
            expo.astype(jnp.bfloat16),
            value_part,
            preferred_element_type=jnp.float32,
        )
        return (new_max, new_sum, new_acc)

    initial = (
        jnp.full((2, local_heads, tok_rows), -1e30, jnp.float32),
        jnp.zeros((2, local_heads, tok_rows), jnp.float32),
        jnp.zeros((2, local_heads, tok_rows, VD), jnp.float32),
    )
    key_rows = lax.all_gather(keys, "sp", axis=0, tiled=True)
    value_rows = lax.all_gather(values, "sp", axis=0, tiled=True)
    key_count = key_rows.shape[0]
    key_span = key_count
    while key_span > 1024 and key_span % 2 == 0:
        key_span = key_span // 2

    def one_span(span_index, inner_state):
        span_start = span_index * key_span
        key_part = lax.dynamic_slice_in_dim(key_rows, span_start, key_span, 0).reshape(
            key_span, local_heads, 2, QK
        )
        value_part = lax.dynamic_slice_in_dim(value_rows, span_start, key_span, 0).reshape(
            key_span, local_heads, VD
        )
        key_pos = span_start + lax.iota(jnp.int32, key_span)
        return update(inner_state, key_part, value_part, key_pos)

    final_max, final_sum, final_acc = lax.fori_loop(0, key_count // key_span, one_span, initial)
    ratio = final_acc / final_sum[..., None]
    mixed_heads = ratio[0] - lambdas[:, None, None] * ratio[1]
    head_out = (
        mixed_heads
        * lax.rsqrt(jnp.mean(mixed_heads * mixed_heads, axis=-1, keepdims=True) + 1e-05)
        * head_gain
    ).astype(jnp.bfloat16)
    out_three = out_weight.reshape(local_heads, VD, model_width)
    own_count = tok_rows // lax.axis_size("tp")
    branch = lax.psum_scatter(
        jnp.einsum("hqd,hde->qe", head_out, out_three, preferred_element_type=jnp.float32).astype(
            jnp.bfloat16
        ),
        "tp",
        scatter_dimension=0,
        tiled=True,
    ).astype(jnp.float32)
    resid_own = lax.dynamic_slice_in_dim(resid, lax.axis_index("tp") * own_count, own_count, 0)
    first = resid_own.astype(jnp.float32) + branch
    normed_all = lax.all_gather(rms_rows(first, norm_gain), "tp", axis=0, tiled=True)
    gate_act = jnp.dot(
        normed_all,
        lax.all_gather(gate_weight, "sp", axis=0, tiled=True),
        preferred_element_type=jnp.float32,
    )
    up_act = jnp.dot(
        normed_all,
        lax.all_gather(up_weight, "sp", axis=0, tiled=True),
        preferred_element_type=jnp.float32,
    )
    hidden = (jax.nn.silu(gate_act) * up_act).astype(jnp.bfloat16)
    terms = jnp.dot(
        hidden,
        lax.all_gather(down_weight, "sp", axis=1, tiled=True),
        preferred_element_type=jnp.float32,
    )
    mixer = lax.psum_scatter(
        terms.astype(jnp.bfloat16), "tp", scatter_dimension=0, tiled=True
    ).astype(jnp.float32)
    finished = (first + 0.5 * mixer).astype(jnp.bfloat16)
    return lax.all_gather(finished, "tp", axis=0, tiled=True)


def where_am_i(R):
    s = lax.axis_index("sp")
    return s // R, lax.rem(s, R), lax.axis_index("tp")


def remote(src, dst, send, recv, sp, tp):
    return pltpu.make_async_remote_copy(
        src_ref=src,
        dst_ref=dst,
        send_sem=send,
        recv_sem=recv,
        device_id={"sp": sp, "tp": tp},
        device_id_type=pl.DeviceIdType.MESH,
    )


def greet(peers):
    barrier = pltpu.get_barrier_semaphore()
    for sp, tp in peers:
        pl.semaphore_signal(
            barrier,
            inc=1,
            device_id={"sp": sp, "tp": tp},
            device_id_type=pl.DeviceIdType.MESH,
        )
    pl.semaphore_wait(barrier, len(peers))


def first_block(zz, share):
    return (zz * share) // LANE


def mirror_x(r):
    return r + 1 - 2 * lax.rem(r, 2)


def mirror_y(r):
    return r + 2 - 4 * (lax.rem(r, 4) // 2)


def attention_block(R, T, i, r, q_at, k_at, v_at, lam, gain):
    span = R * T
    query = q_at(i) * jnp.bfloat16(QK**-0.5)
    ratios = []
    for c in range(2):
        part = query[:, c * QK : (c + 1) * QK]

        def fold(n, state, masked):
            run_max, run_sum, run_acc = state
            key = k_at(n)[:, c * QK : (c + 1) * QK]
            scores = lax.dot_general(
                part, key, (((1,), (1,)), ((), ())), preferred_element_type=jnp.float32
            )
            if masked:
                qpos = r * T + lax.broadcasted_iota(jnp.int32, scores.shape, 0)
                kpos = lax.broadcasted_iota(jnp.int32, scores.shape, 1)
                scores = jnp.where(kpos <= qpos, scores, -1e30)
            new_max = jnp.maximum(run_max, jnp.max(scores, axis=-1, keepdims=True))
            expo = jnp.exp(scores - new_max)
            factor = jnp.exp(run_max - new_max)
            new_sum = run_sum * factor + jnp.sum(expo, axis=-1, keepdims=True)
            new_acc = run_acc * factor + jnp.dot(
                expo.astype(jnp.bfloat16), v_at(n), preferred_element_type=jnp.float32
            )
            return new_max, new_sum, new_acc

        state = (
            jnp.full((T, 1), -1e30, jnp.float32),
            jnp.zeros((T, 1), jnp.float32),
            jnp.zeros((T, VD), jnp.float32),
        )
        state = fold(i, state, True)
        state = lax.fori_loop(0, i, lambda n, st: fold(n, st, False), state)
        ratios.append(state[2] / state[1])
    mixed = ratios[0] - lam * ratios[1]
    return (
        mixed * lax.rsqrt(jnp.mean(mixed * mixed, axis=-1, keepdims=True) + 1e-05) * gain
    ).astype(jnp.bfloat16)


def whole_kernel(Z, R, share, width, refs):
    (
        q_in, k_in, v_in, g_in, u_in, d_in, resid_in, w_in, lam, head_gain, norm_gain,
        out,
        q_sc, k_sc, v_sc, g_sc, u_sc, d_sc, resid, w,
        ho, heads, part, got, first, norm_sc, all_sc,
        hidden, terms, cross, sums, landed,
        send1, recv1, send2, recv2, local_sem, ho_sem, swap_sem, ag_sem, core_sem,
        cross_sem, sum_sem, out_sem,
    ) = refs
    ins = (q_in, k_in, v_in, g_in, u_in, d_in)
    outs = (q_sc, k_sc, v_sc, g_sc, u_sc, d_sc)
    z, r, t = where_am_i(R)
    me = z * R + r
    rx, ry = mirror_x(r), mirror_y(r)
    rd = mirror_x(ry)
    T = k_in.shape[0]
    W = g_in.shape[0]
    D = resid_in.shape[1]
    H = T // 2
    ahead = [lax.rem(z + j, Z) for j in range(Z)]
    behind = [lax.rem(z + Z - j, Z) for j in range(Z)]

    def dev(zz, rr):
        return zz * R + rr

    greet(
        [(dev(ahead[j], r), t) for j in range(1, Z)]
        + [(dev(z, rx), t), (dev(z, ry), t), (me, 1 - t)]
    )

    def source(a, zz, h=None):
        ref = ins[a]
        if a == 5:
            start = pl.multiple_of(first_block(zz, share) * LANE, LANE)
            if h is None:
                return ref.at[pl.ds(start, width), :]
            n = width // 2
            return ref.at[pl.ds(pl.multiple_of(start + h * n, 64), n), :]
        if a < 3:
            rows, sl = T, pl.ds(pl.multiple_of(zz * VD, LANE), VD)
        else:
            rows, sl = W, pl.ds(pl.multiple_of(first_block(zz, share) * LANE, LANE), width)
        if h is None:
            return ref.at[:, sl]
        n = rows // 2
        return ref.at[pl.ds(h * n, n), sl]

    def place(a, zz, rr, h=None):
        ref = outs[a]
        if a == 0:
            return ref.at[zz]
        slot = dev(zz, rr)
        if h is None:
            return ref.at[slot]
        n = ref.shape[1] // 2
        return ref.at[slot, pl.ds(h * n, n), :]

    started, locals_ = [], []

    def first_hop(a, j):
        c = remote(
            source(a, ahead[j]), place(a, z, r), send1.at[a, j], recv1.at[a, j], dev(ahead[j], r), t
        )
        c.start()
        started.append(c)

    def arrived(a, j):
        zz = behind[j]
        remote(
            source(a, z), place(a, zz, r), send1.at[a, j], recv1.at[a, j], dev(zz, r), t
        ).wait_recv()

    def keep(src, dst, n):
        c = pltpu.make_async_copy(src, dst, local_sem.at[n])
        c.start()
        locals_.append(c)

    def hop2(a, j, kind, owner, h, target, from_input):
        zz = behind[j]
        src = source(a, z, h) if from_input else place(a, zz, owner, h)
        return remote(
            src,
            place(a, zz, owner, h),
            send2.at[a - 1, j, kind],
            recv2.at[a - 1, j, kind],
            dev(z, target),
            t,
        )

    def wait2(a, j, kind):
        owner = (rx, rx, ry, ry, rd, rd)[kind]
        target = (rx, rx, ry, ry, ry, rx)[kind]
        hop2(a, j, kind, owner, kind % 2, target, False).wait_recv()

    def send_piece(a, j):
        if j:
            arrived(a, j)
        for kind, h, target in ((0, 0, rx), (3, 1, ry), (1, 1, rx), (2, 0, ry)):
            c = hop2(a, j, kind, r, h, target, j == 0)
            c.start()
            started.append(c)

    def forward_piece(a, j):
        wait2(a, j, 0)
        c = hop2(a, j, 4, rx, 0, ry, False)
        c.start()
        started.append(c)
        wait2(a, j, 3)
        c = hop2(a, j, 5, ry, 1, rx, False)
        c.start()
        started.append(c)

    small = [(a, j) for j in range(Z) for a in (1, 2)]
    for j in range(1, Z):
        for a in (1, 2, 0):
            first_hop(a, j)
    for a in (1, 2):
        send_piece(a, 0)
    for a in (3, 4, 5):
        first_hop(a, 1)
    for j in range(2, Z - 1):
        for a in (3, 4):
            first_hop(a, j)
    for a in range(6):
        keep(source(a, z), place(a, z, r), a)
    keep(resid_in, resid, 6)
    keep(w_in, w, 7)
    lag = 2
    for i in range(2, len(small) + lag):
        if i in (2, 4, 6):
            send_piece(2 + i // 2, 0)
        if i < len(small):
            send_piece(*small[i])
        forward_piece(*small[i - lag])
    for j in range(2, Z - 1):
        first_hop(5, j)
    big = [(a, j) for j in range(Z) for a in (3, 4, 5)]
    big_lag = 3

    def service(i):
        if 3 <= i < len(big):
            send_piece(*big[i])
        if big_lag <= i < len(big) + big_lag:
            forward_piece(*big[i - big_lag])

    for i in range(3, 6):
        service(i)

    for a, j in small:
        for kind in (1, 2, 4, 5):
            wait2(a, j, kind)
    for j in range(1, Z):
        arrived(0, j)
    for c in locals_:
        c.wait()

    head_lam = lam[z]

    def span(ref, n):
        return ref[pl.ds(n * R, R)].reshape(R * T, VD)

    @pl.loop(0, Z)
    def _(i):
        ho[i] = attention_block(
            R,
            T,
            i,
            r,
            lambda b: q_sc[b],
            lambda n: span(k_sc, n),
            lambda n: span(v_sc, n),
            head_lam,
            head_gain[...],
        )

    copies = []
    for j in range(1, Z):
        c = remote(
            ho.at[ahead[j]], heads.at[z], ho_sem.at[0, j], ho_sem.at[1, j], dev(ahead[j], r), t
        )
        c.start()
        copies.append(c)
    for a in (3, 4, 5):
        first_hop(a, Z - 1)
    heads[z] = ho[z]

    for i in range(6, 6 + LATE):
        service(i)

    for c in copies:
        c.wait()
    NT = 512 if D % 512 == 0 else D
    for h in range(2):
        hh = (1 - t) if h == 0 else t
        rows = pl.ds(pl.multiple_of(hh * H, 16), H)
        left = jnp.concatenate([heads[n, rows, :] for n in range(Z)], axis=1)
        for n in range(0, D, NT):
            part[h, :, n : n + NT] = jnp.dot(
                left, w[:, n : n + NT], preferred_element_type=jnp.float32
            ).astype(jnp.bfloat16)
        if h == 0:
            swap = remote(part.at[0], got, swap_sem.at[0], swap_sem.at[1], me, 1 - t)
            swap.start()
    swap.wait()
    own_rows = pl.ds(pl.multiple_of(t * H, 16), H)
    first_val = resid[own_rows, :].astype(jnp.float32) + (
        part[1].astype(jnp.float32) + got[...].astype(jnp.float32)
    )
    first[...] = first_val
    norm_sc[...] = rms_rows(first_val, norm_gain[...])

    def rows_of(zz, tt):
        return all_sc.at[zz, tt]

    def ag_hop(down, d):
        zz = z + (d - 1) if down else z - (d - 1)
        to = z - 1 if down else z + 1
        return remote(
            norm_sc if d == 1 else rows_of(zz, t),
            rows_of(zz, t),
            ag_sem.at[2 * down, d],
            ag_sem.at[2 * down + 1, d],
            dev(to, r),
            t,
        )

    def sends(down, d):
        return (z > 0) & (z + (d - 1) < Z) if down else (z + 1 < Z) & (z - (d - 1) >= 0)

    def gets(down, d):
        return z + d < Z if down else z - d >= 0

    def origin(down, d):
        return z + d if down else z - d

    def to_core(down, d, tt):
        rows = rows_of(origin(down, d), tt)
        n = 2 * d + down
        return remote(rows, rows, core_sem.at[0, n], core_sem.at[1, n], me, 1 - t)

    def ag_start(d):
        for down in (0, 1):

            @pl.when(sends(down, d))
            def _(down=down):
                ag_hop(down, d).start()

    def ag_step(d):
        for down in (0, 1):

            @pl.when(gets(down, d))
            def _(down=down):
                rows = rows_of(origin(down, d), t)
                remote(
                    rows, rows, ag_sem.at[2 * down, d], ag_sem.at[2 * down + 1, d], me, 1 - t
                ).wait_recv()
                if d < Z - 1:

                    @pl.when(sends(down, d + 1))
                    def _():
                        ag_hop(down, d + 1).start()

                to_core(down, d, t).start()

    ag_start(1)
    across = remote(norm_sc, rows_of(z, t), core_sem.at[0, 0], core_sem.at[1, 0], me, 1 - t)
    across.start()
    own = pltpu.make_async_copy(norm_sc, rows_of(z, t), local_sem.at[0])
    own.start()

    for i in range(6 + LATE, len(big)):
        service(i)
    done = 1
    for i in range(len(big), len(big) + big_lag):
        if done < Z:
            ag_step(done)
            done += 1
        service(i)
    for d in range(done, Z):
        ag_step(d)
    own.wait()
    for a, j in big:
        for kind in (1, 2, 4, 5):
            wait2(a, j, kind)
    across.wait_send()
    remote(
        norm_sc, rows_of(z, 1 - t), core_sem.at[0, 0], core_sem.at[1, 0], me, 1 - t
    ).wait_recv()
    for d in range(1, Z):
        for down in (0, 1):

            @pl.when(gets(down, d))
            def _(down=down, d=d):
                to_core(down, d, 1 - t).wait_recv()
                to_core(down, d, t).wait_send()

            @pl.when(sends(down, d))
            def _(down=down, d=d):
                ag_hop(down, d).wait_send()

    FT = 256 if width % 256 == 0 else LANE
    DN = d_sc.shape[2]
    low = first_block(z, share) * LANE
    sent = []
    order = [j % Z for j in range(1, Z + 1)]
    for n, j in enumerate(order):
        zz = ahead[j]
        block = all_sc[zz].reshape(T, D)

        @pl.loop(0, width // FT)
        def _(f, block=block):
            cols = pl.ds(pl.multiple_of(f * FT, FT), FT)
            gate = jnp.dot(
                block, g_sc[:, :, cols].reshape(D, FT), preferred_element_type=jnp.float32
            )
            up = jnp.dot(
                block, u_sc[:, :, cols].reshape(D, FT), preferred_element_type=jnp.float32
            )
            unit = low + f * FT + lax.broadcasted_iota(jnp.int32, gate.shape, 1)
            counted = (unit >= z * share) & (unit < (z + 1) * share)
            value = jax.nn.silu(gate) * up
            hidden[:, cols] = jnp.where(counted, value, 0.0).astype(jnp.bfloat16)

        left = hidden[...]

        @pl.loop(0, (Z * R) // 2)
        def _(p, left=left, n=n):
            right = jnp.concatenate([d_sc[2 * p], d_sc[2 * p + 1]], axis=1)
            value = jnp.dot(left, right, preferred_element_type=jnp.float32).astype(jnp.bfloat16)
            cols = pl.ds(pl.multiple_of(p * (2 * DN), 2 * DN), 2 * DN)
            terms[n, :, :, cols] = value.reshape(2, H, 2 * DN)

        c = remote(
            terms.at[n, 1 - t], cross.at[n], cross_sem.at[0, n], cross_sem.at[1, n], me, 1 - t
        )
        c.start()
        c.wait()
        total = terms[n, t].astype(jnp.float32) + cross[n].astype(jnp.float32)
        if j:
            sums[j] = total.astype(jnp.bfloat16)
            c = remote(
                sums.at[j], landed.at[j], sum_sem.at[0, j], sum_sem.at[1, j], dev(zz, r), t
            )
            c.start()
            sent.append(c)
        else:
            first[...] = first[...] + 0.5 * total
    for c in sent:
        c.wait()
    total = landed[1].astype(jnp.float32)
    for j in range(2, Z):
        total = total + landed[j].astype(jnp.float32)
    sums[0] = (first[...] + 0.5 * total).astype(jnp.bfloat16)
    c = remote(sums.at[0], out.at[own_rows, :], out_sem.at[0], out_sem.at[1], me, 1 - t)
    c.start()
    own = pltpu.make_async_copy(sums.at[0], out.at[own_rows, :], local_sem.at[1])
    own.start()
    own.wait()
    c.wait()
    for c in started:
        c.wait_send()


def columns_form(
    resid,
    queries,
    keys,
    values,
    lambdas,
    head_gain,
    out_weight,
    norm_gain,
    gate_weight,
    up_weight,
    down_weight,
):
    Z = lambdas.shape[0]
    S = lax.axis_size("sp")
    R = S // Z
    T, D = resid.shape
    H = T // 2
    W = gate_weight.shape[0]
    DN = down_weight.shape[1]
    share = gate_weight.shape[1] // Z
    width = LANE * max(
        -(-((zz + 1) * share) // LANE) - (zz * share) // LANE for zz in range(Z)
    )
    bf, f32 = jnp.bfloat16, jnp.float32
    vm = pl.BlockSpec(memory_space=pltpu.VMEM)
    hbm = pl.BlockSpec(memory_space=pl.ANY)
    dma = pltpu.SemaphoreType.DMA

    def kernel(*refs):
        whole_kernel(Z, R, share, width, refs)

    return pl.pallas_call(
        kernel,
        out_shape=jax.ShapeDtypeStruct((T, D), bf),
        in_specs=[hbm] * 8 + [pl.BlockSpec(memory_space=pltpu.SMEM), vm, vm],
        out_specs=vm,
        scratch_shapes=[
            pltpu.VMEM((Z, T, VD), bf),
            pltpu.VMEM((S, T, VD), bf),
            pltpu.VMEM((S, T, VD), bf),
            pltpu.VMEM((S, W, width), bf),
            pltpu.VMEM((S, W, width), bf),
            pltpu.VMEM((S, width, DN), bf),
            pltpu.VMEM((T, D), bf),
            pltpu.VMEM(out_weight.shape, bf),
            pltpu.VMEM((Z, T, VD), bf),
            pltpu.VMEM((Z, T, VD), bf),
            pltpu.VMEM((2, H, D), bf),
            pltpu.VMEM((H, D), bf),
            pltpu.VMEM((H, D), f32),
            pltpu.VMEM((H, D), bf),
            pltpu.VMEM((Z, 2, H, D), bf),
            pltpu.VMEM((T, width), bf),
            pltpu.VMEM((Z, 2, H, D), bf),
            pltpu.VMEM((Z, H, D), bf),
            pltpu.VMEM((Z, H, D), bf),
            pltpu.VMEM((Z, H, D), bf),
            dma((6, Z)),
            dma((6, Z)),
            dma((5, Z, 6)),
            dma((5, Z, 6)),
            dma((8,)),
            dma((2, Z)),
            dma((2,)),
            dma((4, Z)),
            dma((2, 2 * Z)),
            dma((2, Z)),
            dma((2, Z)),
            dma((2,)),
        ],
        compiler_params=pltpu.CompilerParams(
            collective_id=0, has_side_effects=True, vmem_limit_bytes=VMEM_LIMIT
        ),
    )(
        queries,
        keys,
        values,
        gate_weight,
        up_weight,
        down_weight,
        resid,
        out_weight,
        lambdas,
        head_gain.reshape(1, -1),
        norm_gain.reshape(1, -1),
    )


def solution(mesh):
    sp, tp = mesh.shape["sp"], mesh.shape["tp"]

    def local(*args):
        heads = args[4].shape[0]
        tok_rows = args[1].shape[0]
        columns = (
            tp == 2
            and heads > 2
            and sp == 4 * heads
            and args[10].shape[1] % LANE == 0
            and args[8].shape[1] % (16 * heads) == 0
            and tok_rows % 32 == 0
        )
        return (columns_form if columns else generic)(*args)

    return jax.shard_map(
        local,
        mesh=mesh,
        in_specs=(
            P("sp", None),
            P("sp", "tp"),
            P("sp", "tp"),
            P("sp", "tp"),
            P("tp"),
            P(),
            P("tp", None),
            P(),
            P("sp", "tp"),
            P("sp", "tp"),
            P("tp", "sp"),
        ),
        out_specs=P("sp", None),
        check_vma=False,
    )
```
